128 devices in a mesh: ep: 128 (over z, y, x, core).
Axes of the slice: x: 4, y: 4, z: 4, core: 2. Of those that a mesh axis runs over, the one named last changes fastest.
Arguments:
- tokens: bfloat16 [8192, 2048], P('ep'), may hold values from -6 to 6
- conv_state: bfloat16 [8192, 3, 1024], P('ep'), may hold values from -6 to 6
- recur_state: float32 [8192, 1024], P('ep'), may hold values from -6 to 6
- w_branch: bfloat16 [2048, 1024], replicated, may hold values from -0.125 to 0.125
- w_gate: bfloat16 [2048, 1024], replicated, may hold values from -0.125 to 0.125
- conv_taps: float32 [4, 1024], replicated, may hold values from -3 to 3
- rate_blocks: bfloat16 [16, 64, 64], replicated, may hold values from -0.75 to 0.75
- input_blocks: bfloat16 [16, 64, 64], replicated, may hold values from -0.75 to 0.75
- decay_param: float32 [1024], replicated, may hold values from 1.5 to 6.5
- w_mix: bfloat16 [1024, 2048], replicated, may hold values from -0.1875 to 0.1875
- gain_pre: float32 [2048], replicated, may hold values from 0.1 to 1.9
- gain_post: float32 [2048], replicated, may hold values from 0.1 to 1.9
- gain_ffn: float32 [2048], replicated, may hold values from 0.1 to 1.9
- gain_out: float32 [2048], replicated, may hold values from 0.1 to 1.9
- routes: int32 [8192, 2], P('ep'), may hold values from 0 to 127, all different within a row; in each aligned block of 64 rows (0 to 63, 64 to 127, ...) at most 3 rows name the same one
- affinity: float32 [8192, 2], P('ep'), may hold values from 0.05 to 1
- w_expert_gate: bfloat16 [128, 2048, 512], P('ep'), may hold values from -0.125 to 0.125
- w_expert_up: bfloat16 [128, 2048, 512], P('ep'), may hold values from -0.125 to 0.125
- w_expert_down: bfloat16 [128, 512, 2048], P('ep'), may hold values from -0.25 to 0.25
Outputs:
- layer_out: bfloat16 [8192, 2048], P('ep')
- conv_next: bfloat16 [8192, 3, 1024], P('ep')
- state_next: float32 [8192, 1024], P('ep')
The draws below stay inside these ranges and needn't reach their ends.
Inputs may be any that keep to these rules, and one draw needn't show every extreme that they name: `routes`: each row names 2 different experts. Among the 64 rows of one device no expert is named more than 3 times, and in every draw some device names some expert exactly 3 times.
All inputs are finite; a program needn't handle non-finite values.
Results may differ from the reference program's by a relative error of at most 0.014.
Values may be sent and summed in bfloat16 or wider, within the bound.
A program may use at most 128 MiB of HBM per device.

```python
import math
import jax
import jax.numpy as jnp
import numpy as np
from jax import lax

D = 2048
BW = 1024
NB = 16
BS = 64
TAPS = 4
FF = 512
TOP_K = 2
SEQ_DEV = 64
TOKENS = 8192
EXPERTS = 128
CAP = 3
LIMIT = 64


def block_scale(own_key, extent, cuts, least, largest):
    def one(position, parts):
        heights = jax.random.uniform(jax.random.fold_in(jax.random.fold_in(own_key, 6), position), (parts,), jnp.float32, least / len(cuts), largest / len(cuts))
        return jnp.repeat(jnp.exp(heights), extent[position] // parts).reshape((-1,) + (1,) * (len(extent) - position - 1))

    factor_of = one(*cuts[0])
    for cut in cuts[1:]:
        factor_of = factor_of * one(*cut)
    return factor_of


def deal_out(key, own, number, rows, count, top, reach, slope):
    sequence = jax.random.permutation(key, count)
    packed, common = portions_of(count, rows * top, reach, slope, True), portions_of(count, rows * top, reach, slope, False)
    places = jnp.arange(count)

    def named(lengths, offset_by):
        used = int((lengths > 0).sum())
        fixed = max(1, used // 4)
        passed = fixed + (places - fixed + offset_by * (used - fixed)) % max(1, count - fixed)
        return jnp.zeros((count,), jnp.int32).at[sequence[jnp.where(places < fixed, places, passed)]].set(jnp.asarray(lengths, jnp.int32))

    lengths = jnp.where(number % 4 == 0, named(packed, number // 4), named(common, number - number // 4 - 1))
    mixed = jax.random.permutation(jax.random.fold_in(own, 3), count)
    donor, sink = mixed[0:count // 2 * 2:2], mixed[1:count // 2 * 2:2]
    margin = jnp.minimum(lengths[donor] - 1, reach - lengths[sink]) // 2
    margin = jnp.where((donor == sequence[0]) | (sink == sequence[0]) | (lengths[sink] == 0), 0, jnp.maximum(margin, 0))
    passed = jax.random.randint(jax.random.fold_in(own, 4), (count // 2,), 0, 1 << 20) % (margin + 1)
    lengths = lengths.at[donor].add(-passed).at[sink].add(passed)
    labels = jnp.searchsorted(jnp.cumsum(lengths), jnp.arange(rows * top), side="right").astype(jnp.int32)
    listing = labels.reshape(top, rows).T
    listing = listing[jax.random.permutation(jax.random.fold_in(own, 1), rows)]
    offset_by = jax.random.randint(jax.random.fold_in(own, 2), (rows, 1), 0, top)
    return jnp.take_along_axis(listing, (jnp.arange(top)[None, :] + offset_by) % top, axis=1)


def portions_of(count, total, reach, skew, full):
    portions = [(1 << 20) // math.isqrt(standing ** skew) + 1 for standing in range(1, count + 1)]
    largest = reach if full else min(reach, max(-(-total // count), total * portions[0] // sum(portions)))
    least = 1 if total - largest >= count - 1 else 0
    given, surplus = [largest] + [least] * (count - 1), total - largest - least * (count - 1)
    while surplus > 0:
        movable = [i for i in range(1, count) if given[i] < largest] or [i for i in range(1, count) if given[i] < reach]
        whole, left = sum([portions[i] for i in movable]), surplus
        for i in movable:
            more = min(reach - given[i], max(1, left * portions[i] // whole), surplus)
            given[i] = given[i] + more
            surplus = surplus - more
    return np.array(given)


def gaussian(own_key, dims, deviation, limit, shards=(), kind=jnp.bfloat16):
    values = jax.random.normal(own_key, dims, jnp.float32) * deviation
    if len(shards) > 0:
        values = block_scale(own_key, dims, shards, -0.22, 0.18) * values
    return jnp.clip(values, min=-limit, max=limit).astype(kind)


def setup_inputs(seed: int = 0) -> dict:
    streams_of = jax.random.split(jax.random.key(seed), 20)
    tokens = gaussian(streams_of[0], (TOKENS, D), 1.0, 6.0, ((0, 128),))
    conv_state = gaussian(streams_of[1], (TOKENS, TAPS - 1, BW), 1.0, 6.0, ((0, 128),))
    recur_state = gaussian(streams_of[2], (TOKENS, BW), 1.0, 6.0, ((0, 128),), jnp.float32)
    w_branch = gaussian(streams_of[3], (D, BW), D ** -0.5, 0.125)
    w_gate = gaussian(streams_of[4], (D, BW), D ** -0.5, 0.125)
    conv_taps = gaussian(streams_of[5], (TAPS, BW), TAPS ** -0.5, 3.0, (), jnp.float32)
    rate_blocks = gaussian(streams_of[6], (NB, BS, BS), BS ** -0.5, 0.75)
    input_blocks = gaussian(streams_of[7], (NB, BS, BS), BS ** -0.5, 0.75)
    decay_param = jnp.clip(jax.random.uniform(streams_of[8], (BW,), jnp.float32, 1.5, 6.5), 1.5, 6.5)
    w_mix = gaussian(streams_of[9], (BW, D), BW ** -0.5, 0.1875)
    gain_pre = jnp.clip(1.0 + 0.18 * jax.random.normal(streams_of[10], (D,), jnp.float32), 0.1, 1.9)
    gain_post = jnp.clip(1.0 + 0.18 * jax.random.normal(streams_of[11], (D,), jnp.float32), 0.1, 1.9)
    gain_ffn = jnp.clip(1.0 + 0.18 * jax.random.normal(streams_of[12], (D,), jnp.float32), 0.1, 1.9)
    gain_out = jnp.clip(1.0 + 0.18 * jax.random.normal(streams_of[13], (D,), jnp.float32), 0.1, 1.9)
    routes_keys = jax.random.split(jax.random.fold_in(streams_of[14], 1), TOKENS // SEQ_DEV)
    routes_turns = jax.random.permutation(jax.random.fold_in(streams_of[14], 3), TOKENS // SEQ_DEV)
    routes = jax.vmap(lambda own, number: deal_out(jax.random.fold_in(streams_of[14], 2), own, number, SEQ_DEV, EXPERTS, TOP_K, CAP, 2))(routes_keys, routes_turns).reshape((TOKENS, TOP_K))
    affinity = jnp.clip(jnp.exp(math.log(1.0) - 2.9957323 * jax.random.uniform(streams_of[15], (TOKENS, TOP_K), jnp.float32) ** block_scale(streams_of[15], (TOKENS, TOP_K), ((0, 128),), -0.2, 0.2)), 0.05, 1.0)
    w_expert_gate = gaussian(streams_of[16], (EXPERTS, D, FF), D ** -0.5, 0.125, ((0, 128),))
    w_expert_up = gaussian(streams_of[17], (EXPERTS, D, FF), D ** -0.5, 0.125, ((0, 128),))
    w_expert_down = gaussian(streams_of[18], (EXPERTS, FF, D), FF ** -0.5, 0.25, ((0, 128),))
    return dict(tokens=tokens, conv_state=conv_state, recur_state=recur_state, w_branch=w_branch, w_gate=w_gate, conv_taps=conv_taps, rate_blocks=rate_blocks, input_blocks=input_blocks, decay_param=decay_param, w_mix=w_mix, gain_pre=gain_pre, gain_post=gain_post, gain_ffn=gain_ffn, gain_out=gain_out, routes=routes, affinity=affinity, w_expert_gate=w_expert_gate, w_expert_up=w_expert_up, w_expert_down=w_expert_down)


epsilon = 1e-06
gate_scale = 8.0

def norm_rows(values, gain_vec):
    floats = values.astype(jnp.float32)
    inv_scale = lax.rsqrt(lax.optimization_barrier(jnp.mean(floats * floats, axis=-1, keepdims=True)) + epsilon)
    return floats * inv_scale * gain_vec.astype(jnp.float32)

def recurrence(tokens, conv_state, recur_state, w_branch, w_gate, conv_taps, rate_blocks, input_blocks, decay_param, w_mix, gain_pre, gain_post):
    normed = norm_rows(tokens, gain_pre).astype(jnp.bfloat16)
    branch = jnp.dot(normed, w_branch, preferred_element_type=jnp.float32).astype(jnp.bfloat16)
    gate_act = jnp.dot(normed, w_gate, preferred_element_type=jnp.float32).astype(jnp.bfloat16)
    window = jnp.concatenate([conv_state, branch[:, None, :]], axis=1)
    convolved = lax.optimization_barrier(jnp.sum(window.astype(jnp.float32) * conv_taps.astype(jnp.float32)[None], axis=1))
    row_count, branch_width = convolved.shape
    blocks = rate_blocks.shape[0]
    pieces = convolved.reshape(row_count, blocks, branch_width // blocks)
    rate_gate = jax.nn.sigmoid(jnp.einsum('snc,ncd->snd', pieces, rate_blocks.astype(jnp.float32)).reshape(row_count, branch_width))
    inflow = jax.nn.sigmoid(jnp.einsum('snc,ncd->snd', pieces, input_blocks.astype(jnp.float32)).reshape(row_count, branch_width))
    log_decay = -gate_scale * rate_gate * jax.nn.softplus(-decay_param.astype(jnp.float32))
    state_next = jnp.exp(log_decay) * recur_state + jnp.sqrt(-jnp.expm1(2.0 * log_decay)) * (inflow * convolved)
    merged = (state_next * jax.nn.gelu(gate_act.astype(jnp.float32))).astype(jnp.bfloat16)
    mix_out = jnp.dot(merged, w_mix, preferred_element_type=jnp.float32).astype(jnp.bfloat16)
    residual = tokens.astype(jnp.float32) + norm_rows(mix_out, gain_post)
    return (residual, window[:, 1:, :], state_next)

def expert_rows(bundle):
    row_block, gate_w, up_w, down_w = bundle
    gate_part = jnp.dot(row_block, gate_w, preferred_element_type=jnp.float32)
    up_part = jnp.dot(row_block, up_w, preferred_element_type=jnp.float32)
    hidden = (jax.nn.silu(gate_part) * up_part).astype(jnp.bfloat16)
    return jnp.dot(hidden, down_w, preferred_element_type=jnp.float32).astype(jnp.bfloat16)

def reference(tokens, conv_state, recur_state, w_branch, w_gate, conv_taps, rate_blocks, input_blocks, decay_param, w_mix, gain_pre, gain_post, gain_ffn, gain_out, routes, affinity, w_expert_gate, w_expert_up, w_expert_down):
    residual, conv_next, state_next = recurrence(tokens, conv_state, recur_state, w_branch, w_gate, conv_taps, rate_blocks, input_blocks, decay_param, w_mix, gain_pre, gain_post)
    ffn_in = norm_rows(residual, gain_ffn).astype(jnp.bfloat16)
    flat_routes = routes.reshape(-1).astype(jnp.int32)
    onehot = (flat_routes[:, None] == jnp.arange(EXPERTS, dtype=jnp.int32)[None, :]).astype(jnp.int32)
    rank_all = lax.optimization_barrier(jnp.sum(jnp.cumsum(onehot, axis=0) * onehot, axis=1)) - 1
    kept_rows = rank_all < LIMIT
    target = jnp.where(kept_rows, flat_routes * LIMIT + rank_all, EXPERTS * LIMIT).astype(jnp.int32)
    repeated = jnp.repeat(ffn_in, TOP_K, axis=0)
    buffer = jnp.zeros((EXPERTS * LIMIT + 1, D), jnp.bfloat16).at[target].set(repeated)
    grouped = buffer[:EXPERTS * LIMIT].reshape(EXPERTS, LIMIT, D)
    outputs = lax.map(expert_rows, (grouped, w_expert_gate, w_expert_up, w_expert_down))
    out_table = jnp.concatenate([outputs.reshape(EXPERTS * LIMIT, D), jnp.zeros((1, D), jnp.bfloat16)], axis=0)
    picked = jnp.take(out_table, target, axis=0).astype(jnp.float32).reshape(TOKENS, TOP_K, D)
    weights = affinity / lax.optimization_barrier(jnp.sum(affinity, axis=1, keepdims=True))
    combined = lax.optimization_barrier(jnp.sum(weights[:, :, None] * picked, axis=1))
    layer_out = (residual + norm_rows(combined, gain_out)).astype(jnp.bfloat16)
    return (layer_out, conv_next, state_next)
```

```python
import functools

import jax
import jax.numpy as jnp
from jax import lax
from jax.experimental import pallas as pl
from jax.experimental.pallas import tpu as pltpu
from jax.sharding import PartitionSpec as P

MESH = pl.DeviceIdType.MESH
EPS = 1e-06
DECAY = 8.0
LIMIT = 64
SLOTS = 3
F32 = jnp.float32
BF16 = jnp.bfloat16
I32 = jnp.int32


def dot(a, b):
    return jnp.dot(a, b, preferred_element_type=F32)


def inv_rms(values):
    return lax.rsqrt(jnp.mean(values * values, axis=-1, keepdims=True) + EPS)


def minus_expm1(y):
    series = y * (1.0 + y * (1 / 2 + y * (1 / 6 + y * (1 / 24 + y * (1 / 120)))))
    return -jnp.where(y > -0.1, series, jnp.exp(y) - 1.0)


def layer_kernel(
    n,
    tokens,
    conv_in,
    recur,
    taps,
    decay,
    rate_b,
    input_b,
    g_pre,
    g_post,
    g_ffn,
    g_out,
    routes,
    affinity,
    wb_hbm,
    wg_hbm,
    wm_hbm,
    eg_hbm,
    eu_hbm,
    ed_hbm,
    out,
    conv_out,
    state_out,
    wb,
    wg,
    wm,
    eg,
    eu,
    ed,
    bd,
    residual,
    tiles32,
    tiles,
    send,
    recv,
    back,
    xb,
    counts,
    all_counts,
    table_v,
    table_s,
    meta_v,
    meta_s,
    weight_v,
    weight_s,
    w_sem,
    t_sem,
    cs_sem,
    cr_sem,
    ps_sem,
    pr_sem,
    bs_sem,
    br_sem,
):
    me = lax.axis_index("ep")
    rows, width = tokens.shape
    chunks = width // 128

    loads = [
        pltpu.make_async_copy(src, dst, w_sem.at[i])
        for i, (src, dst) in enumerate(
            ((wb_hbm, wb), (wg_hbm, wg), (wm_hbm, wm), (eg_hbm, eg), (eu_hbm, eu), (ed_hbm, ed))
        )
    ]
    for load in loads:
        load.start()

    barrier = pltpu.get_barrier_semaphore()

    def greet(i, carry):
        peer = lax.rem(me + i, n)
        pl.semaphore_signal(barrier, inc=1, device_id=(peer,), device_id_type=MESH)
        return carry

    lax.fori_loop(1, n, greet, 0)

    r0, r1 = routes[0:1, :], routes[1:2, :]
    sub = lax.broadcasted_iota(I32, (rows, rows), 0)
    lane = lax.broadcasted_iota(I32, (rows, rows), 1)
    diag = sub == lane

    def column(row):
        return jnp.sum(jnp.where(diag, row, jnp.zeros_like(row)), axis=1, keepdims=True)

    def as_row(col):
        return jnp.sum(jnp.where(diag, col, jnp.zeros_like(col)), axis=0, keepdims=True)

    experts = lax.broadcasted_iota(I32, (rows, n), 1)
    token_of = lax.broadcasted_iota(I32, (rows, n), 0)
    m0, m1 = column(r0) == experts, column(r1) == experts
    both = m0 | m1
    before = dot((lane < sub).astype(F32), both.astype(F32)).astype(I32)
    counts[...] = jnp.sum(both.astype(I32), axis=0, keepdims=True)
    table_v[...] = jnp.zeros_like(table_v)
    for s in range(SLOTS):
        table_v[s : s + 1, :] = jnp.sum(
            jnp.where(both & (before == s), token_of, 0), axis=0, keepdims=True
        )
    for j, m in enumerate((m0, m1)):
        where_at = jnp.sum(jnp.where(m, experts * SLOTS + before, 0), axis=1, keepdims=True)
        table_v[SLOTS + j : SLOTS + j + 1, 0:rows] = as_row(where_at)
    table_copy = pltpu.make_async_copy(table_v, table_s, t_sem)
    table_copy.start()

    spread = (
        lax.broadcasted_iota(I32, (64, 256), 1) % 64 == lax.broadcasted_iota(I32, (64, 256), 0)
    ).astype(BF16)
    keep = (lax.broadcasted_iota(I32, (256, 256), 0) // 64) == (
        lax.broadcasted_iota(I32, (256, 256), 1) // 64
    )
    for k, blocks in enumerate((rate_b, input_b)):
        for g in range(4):
            wide = dot(blocks[256 * g : 256 * (g + 1), :], spread)
            bd[k, g] = jnp.where(keep, wide, 0.0).astype(BF16)

    tok = tokens[...].astype(F32)
    normed = (tok * inv_rms(tok) * g_pre[...]).astype(BF16)
    loads[0].wait()
    branch = dot(normed, wb[...]).astype(BF16)
    conv = branch.astype(F32) * taps[3:4, :]
    for k in range(3):
        conv = conv + conv_in[k].astype(F32) * taps[k : k + 1, :]
    conv_out[0] = conv_in[1]
    conv_out[1] = conv_in[2]
    conv_out[2] = branch
    conv_b = conv.astype(BF16)
    loads[1].wait()
    gate = dot(normed, wg[...]).astype(BF16).astype(F32)
    d = decay[...]
    soft = jnp.maximum(-d, 0.0) + jnp.log1p(jnp.exp(-jnp.abs(d)))
    merged = []
    for g in range(4):
        cols = slice(256 * g, 256 * (g + 1))
        rate = jax.nn.sigmoid(dot(conv_b[:, cols], bd[0, g]))
        inflow = jax.nn.sigmoid(dot(conv_b[:, cols], bd[1, g]))
        log_decay = -DECAY * rate * soft[:, cols]
        state = jnp.exp(log_decay) * recur[:, cols] + jnp.sqrt(minus_expm1(2.0 * log_decay)) * (
            inflow * conv[:, cols]
        )
        state_out[:, cols] = state
        x = gate[:, cols]
        gelu = 0.5 * x * (1.0 + jnp.tanh(0.7978845608028654 * (x + 0.044715 * (x * x * x))))
        merged.append((state * gelu).astype(BF16))
    merged = jnp.concatenate(merged, axis=1)
    loads[2].wait()
    mix = dot(merged, wm[...]).astype(BF16).astype(F32)
    res = tok + mix * inv_rms(mix) * g_post[...]
    residual[...] = res
    ffn = res * inv_rms(res) * g_ffn[...]

    pl.semaphore_wait(barrier, n - 1)

    def send_counts(i, carry):
        peer = lax.rem(me + i, n)
        pltpu.make_async_remote_copy(
            src_ref=counts,
            dst_ref=all_counts.at[pl.ds(me, 1)],
            send_sem=cs_sem,
            recv_sem=cr_sem,
            device_id=(peer,),
            device_id_type=MESH,
        ).start()
        return carry

    lax.fori_loop(1, n, send_counts, 0)
    all_counts[pl.ds(me, 1), :] = counts[...]

    for c in range(chunks):
        tiles32[pl.ds(c, rows, stride=chunks), :] = ffn[:, 128 * c : 128 * (c + 1)]

    def to_tiles(t, carry):
        at = pl.multiple_of(t * chunks, chunks)
        tiles[t] = tiles32[pl.ds(at, chunks), :].astype(BF16)
        return carry

    lax.fori_loop(0, rows, to_tiles, 0, unroll=8)
    table_copy.wait()

    def pick(e, carry):
        for s in range(SLOTS):
            send[e, s] = tiles[jnp.clip(table_s[s, e], 0, rows - 1)]
        return carry

    lax.fori_loop(0, n, pick, 0, unroll=8)

    def exchange(source, target, ssem, rsem):
        def start(i, carry):
            peer = lax.rem(me + lax.rem(i * 5, n), n)
            pltpu.make_async_remote_copy(
                src_ref=source.at[peer],
                dst_ref=target.at[me],
                send_sem=ssem,
                recv_sem=rsem,
                device_id=(peer,),
                device_id_type=MESH,
            ).start()
            return carry

        lax.fori_loop(1, n, start, 0)
        target[me] = source[me]

    def total(buffer, ssem, rsem):
        part = buffer.at[pl.ds(0, n - 1)]
        return pltpu.make_async_remote_copy(
            src_ref=part,
            dst_ref=part,
            send_sem=ssem,
            recv_sem=rsem,
            device_id=(lax.rem(me + 1, n),),
            device_id_type=MESH,
        )

    exchange(send, recv, ps_sem, pr_sem)

    count_sum = total(all_counts, cs_sem, cr_sem)
    count_sum.wait_recv()
    every = all_counts[...]
    sub_n = lax.broadcasted_iota(I32, (n, n), 0)
    lane_n = lax.broadcasted_iota(I32, (n, n), 1)
    own_col = jnp.sum(jnp.where(lane_n == me, every, 0), axis=1, keepdims=True)
    own_row = jnp.sum(jnp.where(lane_n == sub_n, own_col, 0), axis=0, keepdims=True)
    first_col = jnp.sum(jnp.where(lane_n < sub_n, own_row, 0), axis=1, keepdims=True)
    first_row = jnp.sum(jnp.where(sub_n < lane_n, own_col, 0), axis=0, keepdims=True)
    hit = (first_col <= lane_n) & (lane_n < first_col + own_col)
    meta_v[...] = jnp.zeros_like(meta_v)
    meta_v[0:1, :] = jnp.sum(
        jnp.where(hit, SLOTS * sub_n + lane_n - first_col, 0), axis=0, keepdims=True
    )
    for s in range(SLOTS):
        meta_v[1 + s : 2 + s, :] = jnp.minimum(first_row + s, LIMIT - 1)
    meta_copy = pltpu.make_async_copy(meta_v, meta_s, t_sem)
    meta_copy.start()

    base = jnp.sum(jnp.where(sub_n < me, every, 0), axis=0, keepdims=True)
    fits = (base + before) < LIMIT
    a0, a1 = affinity[0:1, :], affinity[1:2, :]
    weight_v[...] = jnp.zeros_like(weight_v)
    for j, (m, a) in enumerate(((m0, a0), (m1, a1))):
        kept = jnp.sum(jnp.where(m & fits, 1.0, 0.0), axis=1, keepdims=True)
        weight_v[j : j + 1, 0:rows] = as_row(kept) * (a / (a0 + a1))
    meta_copy.wait()
    weight_copy = pltpu.make_async_copy(weight_v, weight_s, t_sem)
    weight_copy.start()

    for load in loads[3:]:
        load.wait()
    rows_sum = total(recv, ps_sem, pr_sem)
    rows_sum.wait_recv()

    recv_rows = recv.reshape(n * SLOTS, chunks, 128)

    def accept(r, carry):
        at = pl.multiple_of(r * chunks, chunks)
        tiles32[pl.ds(at, chunks), :] = recv_rows[jnp.clip(meta_s[0, r], 0, n * SLOTS - 1)].astype(F32)
        return carry

    lax.fori_loop(0, LIMIT, accept, 0, unroll=8)
    for c in range(chunks):
        xb[:, 128 * c : 128 * (c + 1)] = tiles32[pl.ds(c, LIMIT, stride=chunks), :].astype(BF16)
    x = xb[...]
    hidden = (jax.nn.silu(dot(x, eg[...])) * dot(x, eu[...])).astype(BF16)
    result = dot(hidden, ed[...])
    for c in range(chunks):
        tiles32[pl.ds(c, LIMIT, stride=chunks), :] = result[:, 128 * c : 128 * (c + 1)]
    lax.fori_loop(0, LIMIT, to_tiles, 0, unroll=8)

    rows_sum.wait_send()

    def give(e, carry):
        for s in range(SLOTS):
            send[e, s] = tiles[jnp.clip(meta_s[1 + s, e], 0, LIMIT - 1)]
        return carry

    lax.fori_loop(0, n, give, 0, unroll=8)
    exchange(send, back, bs_sem, br_sem)
    weight_copy.wait()
    back_sum = total(back, bs_sem, br_sem)
    back_sum.wait_recv()

    back_rows = back.reshape(n * SLOTS, chunks, 128)

    def combine(t, carry):
        first = back_rows[jnp.clip(table_s[SLOTS, t], 0, n * SLOTS - 1)].astype(F32) * weight_s[0, t]
        second = back_rows[jnp.clip(table_s[SLOTS + 1, t], 0, n * SLOTS - 1)].astype(F32) * weight_s[1, t]
        at = pl.multiple_of(t * chunks, chunks)
        tiles32[pl.ds(at, chunks), :] = first + second
        return carry

    lax.fori_loop(0, rows, combine, 0, unroll=8)
    parts = [tiles32[pl.ds(c, rows, stride=chunks), :] for c in range(chunks)]
    combined = jnp.concatenate(parts, axis=1)
    out[...] = (residual[...] + combined * inv_rms(combined) * g_out[...]).astype(BF16)
    back_sum.wait_send()
    count_sum.wait_send()


def shards(
    n,
    tokens,
    conv_state,
    recur_state,
    w_branch,
    w_gate,
    conv_taps,
    rate_blocks,
    input_blocks,
    decay_param,
    w_mix,
    gain_pre,
    gain_post,
    gain_ffn,
    gain_out,
    routes,
    affinity,
    w_expert_gate,
    w_expert_up,
    w_expert_down,
):
    rows, width = tokens.shape
    bw = recur_state.shape[1]
    ff = w_expert_gate.shape[2]
    chunks = width // 128
    vmem = pl.BlockSpec(memory_space=pltpu.VMEM)
    hbm = pl.BlockSpec(memory_space=pl.ANY)
    dma = pltpu.SemaphoreType.DMA
    layer_out, conv_next, state_next = pl.pallas_call(
        functools.partial(layer_kernel, n),
        out_shape=(
            jax.ShapeDtypeStruct((rows, width), BF16),
            jax.ShapeDtypeStruct((3, rows, bw), BF16),
            jax.ShapeDtypeStruct((rows, bw), F32),
        ),
        in_specs=[vmem] * 13 + [hbm] * 6,
        out_specs=(vmem, vmem, vmem),
        scratch_shapes=[
            pltpu.VMEM((width, bw), BF16),
            pltpu.VMEM((width, bw), BF16),
            pltpu.VMEM((bw, width), BF16),
            pltpu.VMEM((width, ff), BF16),
            pltpu.VMEM((width, ff), BF16),
            pltpu.VMEM((ff, width), BF16),
            pltpu.VMEM((2, 4, 256, 256), BF16),
            pltpu.VMEM((rows, width), F32),
            pltpu.VMEM((rows * chunks + chunks, 128), F32),
            pltpu.VMEM((rows, chunks, 128), BF16),
            pltpu.VMEM((n, SLOTS, chunks, 128), BF16),
            pltpu.VMEM((n, SLOTS, chunks, 128), BF16),
            pltpu.VMEM((n, SLOTS, chunks, 128), BF16),
            pltpu.VMEM((LIMIT, width), BF16),
            pltpu.VMEM((1, n), I32),
            pltpu.VMEM((n, n), I32),
            pltpu.VMEM((8, 128), I32),
            pltpu.SMEM((8, 128), I32),
            pltpu.VMEM((8, 128), I32),
            pltpu.SMEM((8, 128), I32),
            pltpu.VMEM((8, 128), F32),
            pltpu.SMEM((8, 128), F32),
            dma((6,)),
            dma,
            dma,
            dma,
            dma,
            dma,
            dma,
            dma,
        ],
        compiler_params=pltpu.CompilerParams(
            collective_id=0, has_side_effects=True, vmem_limit_bytes=60 * 1024 * 1024
        ),
        name="layer",
    )(
        tokens,
        conv_state.transpose(1, 0, 2),
        recur_state,
        conv_taps,
        decay_param.reshape(1, bw),
        rate_blocks.reshape(bw, -1),
        input_blocks.reshape(bw, -1),
        gain_pre.reshape(1, width),
        gain_post.reshape(1, width),
        gain_ffn.reshape(1, width),
        gain_out.reshape(1, width),
        routes.T,
        affinity.T,
        w_branch,
        w_gate,
        w_mix,
        w_expert_gate.reshape(width, ff),
        w_expert_up.reshape(width, ff),
        w_expert_down.reshape(ff, width),
    )
    return (layer_out, conv_next.transpose(1, 0, 2), state_next)


def solution(mesh):
    row, cube, whole = P("ep", None), P("ep", None, None), P()
    return jax.shard_map(
        functools.partial(shards, mesh.shape["ep"]),
        mesh=mesh,
        in_specs=(row, cube, row) + (whole,) * 11 + (row, row, cube, cube, cube),
        out_specs=(row, cube, row),
        check_vma=False,
    )
```

```python
import functools

import jax
import jax.numpy as jnp
from jax import lax
from jax.experimental import pallas as pl
from jax.experimental.pallas import tpu as pltpu
from jax.sharding import PartitionSpec as P

MESH = pl.DeviceIdType.MESH
EPS = 1e-06
DECAY = 8.0
LIMIT = 64
SLOTS = 3
F32 = jnp.float32
BF16 = jnp.bfloat16
I32 = jnp.int32


def dot(a, b):
    return jnp.dot(a, b, preferred_element_type=F32)


def inv_rms(values):
    return lax.rsqrt(jnp.mean(values * values, axis=-1, keepdims=True) + EPS)


def minus_expm1(y):
    series = y * (1.0 + y * (1 / 2 + y * (1 / 6 + y * (1 / 24 + y * (1 / 120)))))
    return -jnp.where(y > -0.1, series, jnp.exp(y) - 1.0)


SCOPES = []


def scope(name):
    if SCOPES:
        SCOPES.pop().__exit__(None, None, None)
    if name:
        SCOPES.append(jax.named_scope(name))
        SCOPES[-1].__enter__()


def moved(device, step, sign):
    z, y, x, core = step
    return (
        (((device >> 5) + sign * z) & 3) << 5
        | (((device >> 3) + sign * y) & 3) << 3
        | (((device >> 1) + sign * x) & 3) << 1
        | ((device & 1) ^ core)
    )


def step_of(half, q):
    return ((q >> 5) * 2 + (1 - half), (q >> 3) & 3, (q >> 1) & 3, q & 1)


HALF = 64
GROUP = 8
TURN = 37


def layer_kernel(
    n,
    tokens_h,
    conv_h,
    recur_h,
    taps_h,
    decay_h,
    rate_h,
    input_h,
    g_pre_h,
    g_post_h,
    g_ffn_h,
    g_out_h,
    routes_h,
    affinity_h,
    wb_h,
    wg_h,
    wm_h,
    eg_h,
    eu_h,
    ed_h,
    out,
    conv_out,
    state_out,
    tokens,
    conv_in,
    recur,
    taps,
    decay,
    rate_b,
    input_b,
    g_pre,
    g_post,
    g_ffn,
    g_out,
    routes,
    affinity,
    wb,
    wg,
    wm,
    eg,
    eu,
    ed,
    branch_v,
    state_v,
    bd,
    residual,
    tiles32,
    tiles,
    send,
    recv_a,
    recv_b,
    ret_a,
    ret_b,
    back,
    xb,
    counts,
    all_counts,
    table_v,
    table_s,
    meta_v,
    meta_s,
    weight_v,
    weight_s,
    w_sem,
    o_sem,
    t_sem,
    cs_sem,
    cr_sem,
    ps_sem,
    pr_sem,
    bs_sem,
    br_sem,
):
    me = lax.axis_index("ep")
    rows, width = tokens.shape
    chunks = width // 128

    names = dict(
        routes=(routes_h, routes),
        tokens=(tokens_h, tokens),
        g_pre=(g_pre_h, g_pre),
        rate=(rate_h, rate_b),
        input=(input_h, input_b),
        wb=(wb_h, wb),
        conv=(conv_h, conv_in),
        taps=(taps_h, taps),
        wg=(wg_h, wg),
        decay=(decay_h, decay),
        recur=(recur_h, recur),
        wm=(wm_h, wm),
        g_post=(g_post_h, g_post),
        g_ffn=(g_ffn_h, g_ffn),
        affinity=(affinity_h, affinity),
        g_out=(g_out_h, g_out),
        eg=(eg_h, eg),
        eu=(eu_h, eu),
        ed=(ed_h, ed),
    )
    loads = {
        k: pltpu.make_async_copy(src, dst, w_sem.at[i])
        for i, (k, (src, dst)) in enumerate(names.items())
    }
    for load in loads.values():
        load.start()

    def ready(*keys):
        for k in keys:
            loads[k].wait()

    scope("greet")
    barrier = pltpu.get_barrier_semaphore()

    def greet(i, carry):
        for j in range(4):
            peer = (me + 4 * i + j) & (n - 1)
            pl.semaphore_signal(barrier, inc=1, device_id=(peer,), device_id_type=MESH)
        return carry

    lax.fori_loop(1, n // 4, greet, 0)
    for j in range(1, 4):
        peer = (me + j) & (n - 1)
        pl.semaphore_signal(barrier, inc=1, device_id=(peer,), device_id_type=MESH)

    scope("tables")
    ready("routes")
    r0, r1 = routes[0:1, :], routes[1:2, :]
    sub = lax.broadcasted_iota(I32, (rows, rows), 0)
    lane = lax.broadcasted_iota(I32, (rows, rows), 1)
    diag = sub == lane

    def column(row):
        return jnp.sum(jnp.where(diag, row, jnp.zeros_like(row)), axis=1, keepdims=True)

    def as_row(col):
        return jnp.sum(jnp.where(diag, col, jnp.zeros_like(col)), axis=0, keepdims=True)

    experts = lax.broadcasted_iota(I32, (rows, n), 1)
    token_of = lax.broadcasted_iota(I32, (rows, n), 0)
    m0, m1 = column(r0) == experts, column(r1) == experts
    both = m0 | m1
    before = dot((lane < sub).astype(F32), both.astype(F32)).astype(I32)
    counts[...] = jnp.sum(both.astype(I32), axis=0, keepdims=True)
    table_v[...] = jnp.zeros_like(table_v)
    for s in range(SLOTS):
        table_v[s : s + 1, :] = jnp.sum(
            jnp.where(both & (before == s), token_of, 0), axis=0, keepdims=True
        )
    for j, m in enumerate((m0, m1)):
        where_at = jnp.sum(jnp.where(m, experts * SLOTS + before, 0), axis=1, keepdims=True)
        table_v[SLOTS + j : SLOTS + j + 1, 0:rows] = as_row(where_at)
    table_copy = pltpu.make_async_copy(table_v, table_s, t_sem)
    table_copy.start()

    scope("blocks")
    ready("rate", "input")
    spread = (
        lax.broadcasted_iota(I32, (64, 256), 1) % 64 == lax.broadcasted_iota(I32, (64, 256), 0)
    ).astype(BF16)
    keep = (lax.broadcasted_iota(I32, (256, 256), 0) // 64) == (
        lax.broadcasted_iota(I32, (256, 256), 1) // 64
    )
    for k, blocks in enumerate((rate_b, input_b)):
        for g in range(4):
            wide = dot(blocks[256 * g : 256 * (g + 1), :], spread)
            bd[k, g] = jnp.where(keep, wide, 0.0).astype(BF16)

    scope("norm")
    ready("tokens", "g_pre")
    tok = tokens[...].astype(F32)
    normed = (tok * inv_rms(tok) * g_pre[...]).astype(BF16)
    scope("branch")
    ready("wb")
    branch = dot(normed, wb[...]).astype(BF16)
    branch_v[...] = branch
    ready("conv", "taps")
    conv_copies = [
        pltpu.make_async_copy(src, conv_out.at[i], o_sem.at[i])
        for i, src in enumerate((conv_in.at[1], conv_in.at[2], branch_v))
    ]
    for copy in conv_copies:
        copy.start()
    conv = branch.astype(F32) * taps[3:4, :]
    for k in range(3):
        conv = conv + conv_in[k].astype(F32) * taps[k : k + 1, :]
    conv_b = conv.astype(BF16)
    scope("gate")
    ready("wg", "decay", "recur")
    gate = dot(normed, wg[...]).astype(BF16).astype(F32)
    d = decay[...]
    soft = jnp.maximum(-d, 0.0) + jnp.log1p(jnp.exp(-jnp.abs(d)))
    merged = []
    for g in range(4):
        cols = slice(256 * g, 256 * (g + 1))
        rate = jax.nn.sigmoid(dot(conv_b[:, cols], bd[0, g]))
        inflow = jax.nn.sigmoid(dot(conv_b[:, cols], bd[1, g]))
        log_decay = -DECAY * rate * soft[:, cols]
        state = jnp.exp(log_decay) * recur[:, cols] + jnp.sqrt(minus_expm1(2.0 * log_decay)) * (
            inflow * conv[:, cols]
        )
        state_v[:, cols] = state
        x = gate[:, cols]
        gelu = 0.5 * x * (1.0 + jnp.tanh(0.7978845608028654 * (x + 0.044715 * (x * x * x))))
        merged.append((state * gelu).astype(BF16))
    merged = jnp.concatenate(merged, axis=1)
    scope("mix")
    ready("wm", "g_post", "g_ffn")
    mix = dot(merged, wm[...]).astype(BF16).astype(F32)
    res = tok + mix * inv_rms(mix) * g_post[...]
    residual[...] = res
    ffn = res * inv_rms(res) * g_ffn[...]

    scope("tiles")
    for c in range(chunks):
        tiles32[pl.ds(c, rows, stride=chunks), :] = ffn[:, 128 * c : 128 * (c + 1)]

    def to_tiles(t, carry):
        at = pl.multiple_of(t * chunks, chunks)
        tiles[t] = tiles32[pl.ds(at, chunks), :].astype(BF16)
        return carry

    lax.fori_loop(0, rows, to_tiles, 0, unroll=8)
    table_copy.wait()

    scope("barrier")
    pl.semaphore_wait(barrier, n - 1)
    scope("send")

    def own_tile(index):
        return tiles[jnp.clip(index, 0, rows - 1)]

    def turned(i):
        return (i * TURN) & (HALF - 1)

    def post(source, target, ssem, rsem, peer):
        pltpu.make_async_remote_copy(
            src_ref=source,
            dst_ref=target,
            send_sem=ssem,
            recv_sem=rsem,
            device_id=(peer,),
            device_id_type=MESH,
        ).start()

    def send_count(peer):
        post(counts, all_counts.at[pl.ds(me, 1)], cs_sem, cr_sem, peer)

    def piped(first, prepare, launch):
        def group(g, start, run):
            for j in range(start, GROUP):
                run(g * GROUP + j)

        def body(g, carry):
            group(g, 0, prepare)
            group(g - 1, 0, launch)
            return carry

        group(0, first, prepare)
        group(1, 0, prepare)
        group(0, first, launch)
        lax.fori_loop(2, HALF // GROUP, body, 0)
        group(HALF // GROUP - 1, 0, launch)

    def pick_rows(half, i):
        peer = moved(me, step_of(half, turned(i)), 1)
        for s in range(SLOTS):
            send[peer, s] = own_tile(table_s[s, peer])
        if half == 0:
            send_count(peer)
            if not (isinstance(i, int) and i == 0):
                send_count(moved(me, step_of(1, turned(i)), 1))

    def send_rows(half, i):
        q = turned(i)
        peer = moved(me, step_of(half, q), 1)
        target = (recv_a, recv_b)[half]
        post(send.at[peer], target.at[q], ps_sem.at[half], pr_sem.at[half], peer)

    for half in range(2):
        piped(half, functools.partial(pick_rows, half), functools.partial(send_rows, half))
    for s in range(SLOTS):
        recv_b[0, s] = own_tile(table_s[s, me])
    all_counts[pl.ds(me, 1), :] = counts[...]
    state_copy = pltpu.make_async_copy(state_v, state_out, o_sem.at[3])
    state_copy.start()

    def total(buffer, blocks, ssem, rsem):
        part = buffer.at[pl.ds(0, blocks)]
        return pltpu.make_async_remote_copy(
            src_ref=part,
            dst_ref=part,
            send_sem=ssem,
            recv_sem=rsem,
            device_id=(me ^ 1,),
            device_id_type=MESH,
        )

    scope("meta")
    count_sum = total(all_counts, n - 1, cs_sem, cr_sem)
    count_sum.wait_recv()
    every = all_counts[...]
    sub_n = lax.broadcasted_iota(I32, (n, n), 0)
    lane_n = lax.broadcasted_iota(I32, (n, n), 1)
    own_col = jnp.sum(jnp.where(lane_n == me, every, 0), axis=1, keepdims=True)
    own_row = jnp.sum(jnp.where(lane_n == sub_n, own_col, 0), axis=0, keepdims=True)
    first_col = jnp.sum(jnp.where(lane_n < sub_n, own_row, 0), axis=1, keepdims=True)
    first_row = jnp.sum(jnp.where(sub_n < lane_n, own_col, 0), axis=0, keepdims=True)
    hit = (first_col <= lane_n) & (lane_n < first_col + own_col)
    step_z = ((me >> 5) - (sub_n >> 5)) & 3
    entry = (
        (step_z >> 1) << 5
        | (((me >> 3) - (sub_n >> 3)) & 3) << 3
        | (((me >> 1) - (sub_n >> 1)) & 3) << 1
        | ((me ^ sub_n) & 1)
    )
    place = SLOTS * entry + lane_n - first_col
    meta_v[...] = jnp.zeros_like(meta_v)
    for half in range(2):
        meta_v[half : half + 1, :] = jnp.sum(
            jnp.where(hit & ((step_z & 1) == 1 - half), place, 0), axis=0, keepdims=True
        )
    for s in range(SLOTS):
        meta_v[2 + s : 3 + s, :] = jnp.minimum(first_row + s, LIMIT - 1)
    meta_copy = pltpu.make_async_copy(meta_v, meta_s, t_sem)
    meta_copy.start()

    base = jnp.sum(jnp.where(sub_n < me, every, 0), axis=0, keepdims=True)
    fits = (base + before) < LIMIT
    ready("affinity")
    a0, a1 = affinity[0:1, :], affinity[1:2, :]
    weight_v[...] = jnp.zeros_like(weight_v)
    for j, (m, a) in enumerate(((m0, a0), (m1, a1))):
        kept = jnp.sum(jnp.where(m & fits, 1.0, 0.0), axis=1, keepdims=True)
        weight_v[j : j + 1, 0:rows] = as_row(kept) * (a / (a0 + a1))
    meta_copy.wait()
    weight_copy = pltpu.make_async_copy(weight_v, weight_s, t_sem)
    weight_copy.start()
    ready("eg", "eu", "ed", "g_out")

    sums = []
    for half, (got, ret) in enumerate(((recv_a, ret_a), (recv_b, ret_b))):
        scope(f"wait{half}")
        rows_sum = total(got, HALF - half, ps_sem.at[half], pr_sem.at[half])
        rows_sum.wait_recv()
        sums.append(rows_sum)
        scope(f"expert{half}")
        got_rows = got.reshape(HALF * SLOTS, chunks, 128)

        def accept(r, carry):
            at = pl.multiple_of(r * chunks, chunks)
            index = jnp.clip(meta_s[half, r], 0, HALF * SLOTS - 1)
            tiles32[pl.ds(at, chunks), :] = got_rows[index].astype(F32)
            return carry

        lax.fori_loop(0, LIMIT, accept, 0, unroll=8)
        for c in range(chunks):
            part = tiles32[pl.ds(c, LIMIT, stride=chunks), :]
            xb[:, 128 * c : 128 * (c + 1)] = part.astype(BF16)
        x = xb[...]
        hidden = (jax.nn.silu(dot(x, eg[...])) * dot(x, eu[...])).astype(BF16)
        result = dot(hidden, ed[...])
        for c in range(chunks):
            tiles32[pl.ds(c, LIMIT, stride=chunks), :] = result[:, 128 * c : 128 * (c + 1)]
        lax.fori_loop(0, LIMIT, to_tiles, 0, unroll=8)
        scope(f"give{half}")

        def result_tile(s, peer):
            return tiles[jnp.clip(meta_s[2 + s, peer], 0, LIMIT - 1)]

        def give(i):
            q = turned(i)
            peer = moved(me, step_of(half, q), -1)
            for s in range(SLOTS):
                ret[q, s] = result_tile(s, peer)

        def send_back(i):
            q = turned(i)
            peer = moved(me, step_of(half, q), -1)
            post(ret.at[q], back.at[me], bs_sem, br_sem, peer)

        piped(half, give, send_back)
    for s in range(SLOTS):
        back[me, s] = result_tile(s, me)
    weight_copy.wait()
    scope("wait2")
    back_sum = total(back, n - 1, bs_sem, br_sem)
    back_sum.wait_recv()

    scope("combine")
    back_rows = back.reshape(n * SLOTS, chunks, 128)

    def combine(t, carry):
        first, second = (
            back_rows[jnp.clip(table_s[SLOTS + j, t], 0, n * SLOTS - 1)].astype(F32)
            * weight_s[j, t]
            for j in range(2)
        )
        at = pl.multiple_of(t * chunks, chunks)
        tiles32[pl.ds(at, chunks), :] = first + second
        return carry

    lax.fori_loop(0, rows, combine, 0, unroll=8)
    parts = [tiles32[pl.ds(c, rows, stride=chunks), :] for c in range(chunks)]
    combined = jnp.concatenate(parts, axis=1)
    out[...] = (residual[...] + combined * inv_rms(combined) * g_out[...]).astype(BF16)
    scope("drain")
    for done in sums:
        done.wait_send()
    back_sum.wait_send()
    count_sum.wait_send()
    for copy in (*conv_copies, state_copy):
        copy.wait()
    scope(None)


def deliver_kernel(a, b, c, a_out, b_out, c_out, a_v, b_v, c_v, sem):
    trips = ((a, a_v, a_out), (b, b_v, b_out), (c, c_v, c_out))
    into = [pltpu.make_async_copy(x, v, sem.at[i]) for i, (x, v, _) in enumerate(trips)]
    onward = [pltpu.make_async_copy(v, y, sem.at[3 + i]) for i, (_, v, y) in enumerate(trips)]
    for copy in into:
        copy.start()
    for first, second in zip(into, onward):
        first.wait()
        second.start()
    for copy in onward:
        copy.wait()


def shards(
    n,
    tokens,
    conv_state,
    recur_state,
    w_branch,
    w_gate,
    conv_taps,
    rate_blocks,
    input_blocks,
    decay_param,
    w_mix,
    gain_pre,
    gain_post,
    gain_ffn,
    gain_out,
    routes,
    affinity,
    w_expert_gate,
    w_expert_up,
    w_expert_down,
):
    rows, width = tokens.shape
    bw = recur_state.shape[1]
    ff = w_expert_gate.shape[2]
    chunks = width // 128
    vmem = pl.BlockSpec(memory_space=pltpu.VMEM)
    hbm = pl.BlockSpec(memory_space=pl.ANY)
    dma = pltpu.SemaphoreType.DMA
    inputs = (
        tokens,
        conv_state.transpose(1, 0, 2),
        recur_state,
        conv_taps,
        decay_param.reshape(1, bw),
        rate_blocks.reshape(bw, -1),
        input_blocks.reshape(bw, -1),
        gain_pre.reshape(1, width),
        gain_post.reshape(1, width),
        gain_ffn.reshape(1, width),
        gain_out.reshape(1, width),
        routes.T,
        affinity.T,
        w_branch,
        w_gate,
        w_mix,
        w_expert_gate.reshape(width, ff),
        w_expert_up.reshape(width, ff),
        w_expert_down.reshape(ff, width),
    )
    results = (
        jax.ShapeDtypeStruct((rows, width), BF16),
        jax.ShapeDtypeStruct((3, rows, bw), BF16),
        jax.ShapeDtypeStruct((rows, bw), F32),
    )
    produced = pl.pallas_call(
        functools.partial(layer_kernel, n),
        out_shape=results,
        in_specs=[hbm] * len(inputs),
        out_specs=(vmem, hbm, hbm),
        scratch_shapes=[pltpu.VMEM(x.shape, x.dtype) for x in inputs]
        + [
            pltpu.VMEM((rows, bw), BF16),
            pltpu.VMEM((rows, bw), F32),
            pltpu.VMEM((2, 4, 256, 256), BF16),
            pltpu.VMEM((rows, width), F32),
            pltpu.VMEM((rows * chunks + chunks, 128), F32),
            pltpu.VMEM((rows, chunks, 128), BF16),
            pltpu.VMEM((n, SLOTS, chunks, 128), BF16),
            pltpu.VMEM((HALF, SLOTS, chunks, 128), BF16),
            pltpu.VMEM((HALF, SLOTS, chunks, 128), BF16),
            pltpu.VMEM((HALF, SLOTS, chunks, 128), BF16),
            pltpu.VMEM((HALF, SLOTS, chunks, 128), BF16),
            pltpu.VMEM((n, SLOTS, chunks, 128), BF16),
            pltpu.VMEM((LIMIT, width), BF16),
            pltpu.VMEM((1, n), I32),
            pltpu.VMEM((n, n), I32),
            pltpu.VMEM((8, 128), I32),
            pltpu.SMEM((8, 128), I32),
            pltpu.VMEM((8, 128), I32),
            pltpu.SMEM((8, 128), I32),
            pltpu.VMEM((8, 128), F32),
            pltpu.SMEM((8, 128), F32),
            dma((len(inputs),)),
            dma((4,)),
            dma,
            dma,
            dma,
            dma((2,)),
            dma((2,)),
            dma,
            dma,
        ],
        compiler_params=pltpu.CompilerParams(
            collective_id=0, has_side_effects=True, vmem_limit_bytes=60 * 1024 * 1024
        ),
        name="layer",
    )(*inputs)
    layer_out, conv_next, state_next = pl.pallas_call(
        deliver_kernel,
        out_shape=results,
        in_specs=[hbm] * 3,
        out_specs=(hbm, hbm, hbm),
        scratch_shapes=[pltpu.VMEM(x.shape, x.dtype) for x in results] + [dma((6,))],
        name="deliver",
    )(*produced)
    return (layer_out, conv_next.transpose(1, 0, 2), state_next)


def solution(mesh):
    row, cube, whole = P("ep", None), P("ep", None, None), P()
    return jax.shard_map(
        functools.partial(shards, mesh.shape["ep"]),
        mesh=mesh,
        in_specs=(row, cube, row) + (whole,) * 11 + (row, row, cube, cube, cube),
        out_specs=(row, cube, row),
        check_vma=False,
    )
```

```python
import functools

import jax
import jax.numpy as jnp
from jax import lax
from jax.experimental import pallas as pl
from jax.experimental.pallas import tpu as pltpu
from jax.sharding import PartitionSpec as P

MESH = pl.DeviceIdType.MESH
EPS = 1e-06
DECAY = 8.0
LIMIT = 64
SLOTS = 3
F32 = jnp.float32
BF16 = jnp.bfloat16
I32 = jnp.int32


def dot(a, b):
    return jnp.dot(a, b, preferred_element_type=F32)


def inv_rms(values):
    return lax.rsqrt(jnp.mean(values * values, axis=-1, keepdims=True) + EPS)


def minus_expm1(y):
    series = y * (1.0 + y * (1 / 2 + y * (1 / 6 + y * (1 / 24 + y * (1 / 120)))))
    return -jnp.where(y > -0.1, series, jnp.exp(y) - 1.0)


SCOPES = []


def scope(name):
    if SCOPES:
        SCOPES.pop().__exit__(None, None, None)
    if name:
        SCOPES.append(jax.named_scope(name))
        SCOPES[-1].__enter__()


def moved(device, step, sign):
    z, y, x, core = step
    return (
        (((device >> 5) + sign * z) & 3) << 5
        | (((device >> 3) + sign * y) & 3) << 3
        | (((device >> 1) + sign * x) & 3) << 1
        | ((device & 1) ^ core)
    )


def step_of(half, q):
    return ((q >> 5) * 2 + (1 - half), (q >> 3) & 3, (q >> 1) & 3, q & 1)


HALF = 64
GROUP = 8
TURN = 47


def layer_kernel(
    n,
    tokens_h,
    conv_h,
    recur_h,
    taps_h,
    decay_h,
    rate_h,
    input_h,
    g_pre_h,
    g_post_h,
    g_ffn_h,
    g_out_h,
    routes_h,
    affinity_h,
    wb_h,
    wg_h,
    wm_h,
    eg_h,
    eu_h,
    ed_h,
    out,
    conv_out,
    state_out,
    tokens,
    conv_in,
    recur,
    taps,
    decay,
    rate_b,
    input_b,
    g_pre,
    g_post,
    g_ffn,
    g_out,
    routes,
    affinity,
    wb,
    wg,
    wm,
    eg,
    eu,
    ed,
    bd,
    residual,
    tiles32,
    tiles,
    send,
    recv_a,
    recv_b,
    ret_a,
    ret_b,
    back,
    xb,
    counts,
    all_counts,
    table_v,
    table_s,
    meta_v,
    meta_s,
    weight_v,
    weight_s,
    w_sem,
    t_sem,
    cs_sem,
    cr_sem,
    ps_sem,
    pr_sem,
    bs_sem,
    br_sem,
):
    me = lax.axis_index("ep")
    rows, width = tokens.shape
    chunks = width // 128

    loads = {}

    def load(key, src, dst):
        loads[key] = pltpu.make_async_copy(src, dst, w_sem.at[len(loads)])
        loads[key].start()

    def ready(*keys):
        for k in keys:
            loads[k].wait()

    def load_columns(g):
        cols = pl.ds(256 * g, 256)
        load(f"wb{g}", wb_h.at[:, cols], wb.at[:, cols])
        load(f"wg{g}", wg_h.at[:, cols], wg.at[:, cols])

    load("tokens", tokens_h, tokens)
    load("g_pre", g_pre_h, g_pre)
    load("routes", routes_h, routes)
    load("rate", rate_h, rate_b)
    load("input", input_h, input_b)
    load_columns(0)
    load("conv", conv_h, conv_in)
    load("taps", taps_h, taps)
    load("decay", decay_h, decay)
    load("recur", recur_h, recur)
    load_columns(1)
    load_columns(2)
    load_columns(3)
    for h in range(2):
        part = pl.ds(512 * h, 512)
        load(f"wm{h}", wm_h.at[part], wm.at[part])
    load("g_post", g_post_h, g_post)
    load("g_ffn", g_ffn_h, g_ffn)
    load("affinity", affinity_h, affinity)
    load("g_out", g_out_h, g_out)

    scope("greet")
    barrier = pltpu.get_barrier_semaphore()

    def greet(i, carry):
        for j in range(4):
            peer = (me + 4 * i + j) & (n - 1)
            pl.semaphore_signal(barrier, inc=1, device_id=(peer,), device_id_type=MESH)
        return carry

    lax.fori_loop(1, n // 4, greet, 0)
    for j in range(1, 4):
        peer = (me + j) & (n - 1)
        pl.semaphore_signal(barrier, inc=1, device_id=(peer,), device_id_type=MESH)

    scope("norm")
    ready("tokens", "g_pre", "routes", "rate", "input")
    tok = tokens[...].astype(F32)
    normed = (tok * inv_rms(tok) * g_pre[...]).astype(BF16)
    scope("first")
    ready("wb0", "wg0", "conv", "taps", "decay", "recur")
    spread = (
        lax.broadcasted_iota(I32, (64, 256), 1) % 64 == lax.broadcasted_iota(I32, (64, 256), 0)
    ).astype(BF16)
    keep = (lax.broadcasted_iota(I32, (256, 256), 0) // 64) == (
        lax.broadcasted_iota(I32, (256, 256), 1) // 64
    )
    for k, blocks in enumerate((rate_b, input_b)):
        for g in range(4):
            wide = dot(blocks[256 * g : 256 * (g + 1), :], spread)
            bd[k, g] = jnp.where(keep, wide, 0.0).astype(BF16)

    r0, r1 = routes[0:1, :], routes[1:2, :]
    sub = lax.broadcasted_iota(I32, (rows, rows), 0)
    lane = lax.broadcasted_iota(I32, (rows, rows), 1)
    diag = sub == lane

    def column(row):
        return jnp.sum(jnp.where(diag, row, jnp.zeros_like(row)), axis=1, keepdims=True)

    def as_row(col):
        return jnp.sum(jnp.where(diag, col, jnp.zeros_like(col)), axis=0, keepdims=True)

    experts = lax.broadcasted_iota(I32, (rows, n), 1)
    token_of = lax.broadcasted_iota(I32, (rows, n), 0)
    m0, m1 = column(r0) == experts, column(r1) == experts
    both = m0 | m1
    before = dot((lane < sub).astype(F32), both.astype(F32)).astype(I32)
    counts[...] = jnp.sum(both.astype(I32), axis=0, keepdims=True)
    table_v[...] = jnp.zeros_like(table_v)
    for s in range(SLOTS):
        table_v[s : s + 1, :] = jnp.sum(
            jnp.where(both & (before == s), token_of, 0), axis=0, keepdims=True
        )
    for j, m in enumerate((m0, m1)):
        where_at = jnp.sum(jnp.where(m, experts * SLOTS + before, 0), axis=1, keepdims=True)
        table_v[SLOTS + j : SLOTS + j + 1, 0:rows] = as_row(where_at)
    table_copy = pltpu.make_async_copy(table_v, table_s, t_sem)
    table_copy.start()

    def project(g):
        cols = slice(256 * g, 256 * (g + 1))
        return dot(normed, wb[:, cols]).astype(BF16), dot(normed, wg[:, cols]).astype(BF16)

    def advance(g, branch, gate):
        cols = slice(256 * g, 256 * (g + 1))
        conv_out[0, :, cols] = conv_in[1, :, cols]
        conv_out[1, :, cols] = conv_in[2, :, cols]
        conv_out[2, :, cols] = branch
        conv = branch.astype(F32) * taps[3:4, cols]
        for k in range(3):
            conv = conv + conv_in[k, :, cols].astype(F32) * taps[k : k + 1, cols]
        conv_b = conv.astype(BF16)
        d = decay[:, cols]
        soft = jnp.maximum(-d, 0.0) + jnp.log1p(jnp.exp(-jnp.abs(d)))
        rate = jax.nn.sigmoid(dot(conv_b, bd[0, g]))
        inflow = jax.nn.sigmoid(dot(conv_b, bd[1, g]))
        log_decay = -DECAY * rate * soft
        state = jnp.exp(log_decay) * recur[:, cols] + jnp.sqrt(minus_expm1(2.0 * log_decay)) * (
            inflow * conv
        )
        state_out[:, cols] = state
        x = gate.astype(F32)
        gelu = 0.5 * x * (1.0 + jnp.tanh(0.7978845608028654 * (x + 0.044715 * (x * x * x))))
        return (state * gelu).astype(BF16)

    merged = []
    projected = project(0)
    scope("project")
    for g in range(1, 4):
        ready(f"wb{g}", f"wg{g}")
        following = project(g)
        merged.append(advance(g - 1, *projected))
        projected = following
    scope("mix")
    ready("wm0")
    half_mix = dot(jnp.concatenate(merged[:2], axis=1), wm[:512, :])
    merged.append(advance(3, *projected))
    ready("wm1", "g_post", "g_ffn")
    mix = half_mix + dot(jnp.concatenate(merged[2:], axis=1), wm[512:, :])
    mix = mix.astype(BF16).astype(F32)
    load("eg", eg_h, eg)
    load("eu", eu_h, eu)
    load("ed", ed_h, ed)
    res = tok + mix * inv_rms(mix) * g_post[...]
    residual[...] = res
    ffn = res * inv_rms(res) * g_ffn[...]

    scope("tiles")
    for c in range(chunks):
        tiles32[pl.ds(c, rows, stride=chunks), :] = ffn[:, 128 * c : 128 * (c + 1)]

    def to_tiles(t, carry):
        at = pl.multiple_of(t * chunks, chunks)
        tiles[t] = tiles32[pl.ds(at, chunks), :].astype(BF16)
        return carry

    lax.fori_loop(0, rows, to_tiles, 0, unroll=8)
    table_copy.wait()

    scope("barrier")
    pl.semaphore_wait(barrier, n - 1)
    scope("send")

    def own_tile(index):
        return tiles[jnp.clip(index, 0, rows - 1)]

    def turned(i):
        return (i * TURN) & (HALF - 1)

    def post(source, target, ssem, rsem, peer):
        pltpu.make_async_remote_copy(
            src_ref=source,
            dst_ref=target,
            send_sem=ssem,
            recv_sem=rsem,
            device_id=(peer,),
            device_id_type=MESH,
        ).start()

    def send_count(peer):
        post(counts, all_counts.at[pl.ds(me, 1)], cs_sem, cr_sem, peer)

    def piped(first, prepare, launch):
        def group(g, start, run):
            for j in range(start, GROUP):
                run(g * GROUP + j)

        def body(g, carry):
            group(g, 0, prepare)
            group(g - 1, 0, launch)
            return carry

        group(0, first, prepare)
        group(1, 0, prepare)
        group(0, first, launch)
        lax.fori_loop(2, HALF // GROUP, body, 0)
        group(HALF // GROUP - 1, 0, launch)

    def pick_rows(half, i):
        peer = moved(me, step_of(half, turned(i)), 1)
        for s in range(SLOTS):
            send[peer, s] = own_tile(table_s[s, peer])
        if half == 0:
            send_count(peer)
            if not (isinstance(i, int) and i == 0):
                send_count(moved(me, step_of(1, turned(i)), 1))

    def send_rows(half, i):
        q = turned(i)
        peer = moved(me, step_of(half, q), 1)
        target = (recv_a, recv_b)[half]
        post(send.at[peer], target.at[q], ps_sem.at[half], pr_sem.at[half], peer)

    for half in range(2):
        piped(half, functools.partial(pick_rows, half), functools.partial(send_rows, half))
    for s in range(SLOTS):
        recv_b[0, s] = own_tile(table_s[s, me])
    all_counts[pl.ds(me, 1), :] = counts[...]

    def total(buffer, blocks, ssem, rsem):
        part = buffer.at[pl.ds(0, blocks)]
        return pltpu.make_async_remote_copy(
            src_ref=part,
            dst_ref=part,
            send_sem=ssem,
            recv_sem=rsem,
            device_id=(me ^ 1,),
            device_id_type=MESH,
        )

    scope("meta")
    count_sum = total(all_counts, n - 1, cs_sem, cr_sem)
    count_sum.wait_recv()
    every = all_counts[...]
    sub_n = lax.broadcasted_iota(I32, (n, n), 0)
    lane_n = lax.broadcasted_iota(I32, (n, n), 1)
    own_col = jnp.sum(jnp.where(lane_n == me, every, 0), axis=1, keepdims=True)
    own_row = jnp.sum(jnp.where(lane_n == sub_n, own_col, 0), axis=0, keepdims=True)
    first_col = jnp.sum(jnp.where(lane_n < sub_n, own_row, 0), axis=1, keepdims=True)
    first_row = jnp.sum(jnp.where(sub_n < lane_n, own_col, 0), axis=0, keepdims=True)
    hit = (first_col <= lane_n) & (lane_n < first_col + own_col)
    step_z = ((me >> 5) - (sub_n >> 5)) & 3
    entry = (
        (step_z >> 1) << 5
        | (((me >> 3) - (sub_n >> 3)) & 3) << 3
        | (((me >> 1) - (sub_n >> 1)) & 3) << 1
        | ((me ^ sub_n) & 1)
    )
    place = SLOTS * entry + lane_n - first_col
    meta_v[...] = jnp.zeros_like(meta_v)
    for half in range(2):
        meta_v[half : half + 1, :] = jnp.sum(
            jnp.where(hit & ((step_z & 1) == 1 - half), place, 0), axis=0, keepdims=True
        )
    for s in range(SLOTS):
        meta_v[2 + s : 3 + s, :] = jnp.minimum(first_row + s, LIMIT - 1)
    meta_copy = pltpu.make_async_copy(meta_v, meta_s, t_sem)
    meta_copy.start()

    base = jnp.sum(jnp.where(sub_n < me, every, 0), axis=0, keepdims=True)
    fits = (base + before) < LIMIT
    ready("affinity")
    a0, a1 = affinity[0:1, :], affinity[1:2, :]
    weight_v[...] = jnp.zeros_like(weight_v)
    for j, (m, a) in enumerate(((m0, a0), (m1, a1))):
        kept = jnp.sum(jnp.where(m & fits, 1.0, 0.0), axis=1, keepdims=True)
        weight_v[j : j + 1, 0:rows] = as_row(kept) * (a / (a0 + a1))
    meta_copy.wait()
    weight_copy = pltpu.make_async_copy(weight_v, weight_s, t_sem)
    weight_copy.start()
    ready("eg", "eu", "ed", "g_out")

    sums = []
    for half, (got, ret) in enumerate(((recv_a, ret_a), (recv_b, ret_b))):
        scope(f"wait{half}")
        rows_sum = total(got, HALF - half, ps_sem.at[half], pr_sem.at[half])
        rows_sum.wait_recv()
        sums.append(rows_sum)
        scope(f"expert{half}")
        got_rows = got.reshape(HALF * SLOTS, chunks, 128)

        def accept(r, carry):
            at = pl.multiple_of(r * chunks, chunks)
            index = jnp.clip(meta_s[half, r], 0, HALF * SLOTS - 1)
            tiles32[pl.ds(at, chunks), :] = got_rows[index].astype(F32)
            return carry

        lax.fori_loop(0, LIMIT, accept, 0, unroll=8)
        for c in range(chunks):
            part = tiles32[pl.ds(c, LIMIT, stride=chunks), :]
            xb[:, 128 * c : 128 * (c + 1)] = part.astype(BF16)
        x = xb[...]
        hidden = (jax.nn.silu(dot(x, eg[...])) * dot(x, eu[...])).astype(BF16)
        result = dot(hidden, ed[...])
        for c in range(chunks):
            tiles32[pl.ds(c, LIMIT, stride=chunks), :] = result[:, 128 * c : 128 * (c + 1)]
        lax.fori_loop(0, LIMIT, to_tiles, 0, unroll=8)
        scope(f"give{half}")

        def result_tile(s, peer):
            return tiles[jnp.clip(meta_s[2 + s, peer], 0, LIMIT - 1)]

        def give(i):
            q = turned(i)
            peer = moved(me, step_of(half, q), -1)
            for s in range(SLOTS):
                ret[q, s] = result_tile(s, peer)

        def send_back(i):
            q = turned(i)
            peer = moved(me, step_of(half, q), -1)
            post(ret.at[q], back.at[me], bs_sem, br_sem, peer)

        piped(half, give, send_back)
    for s in range(SLOTS):
        back[me, s] = result_tile(s, me)
    weight_copy.wait()
    scope("wait2")
    back_sum = total(back, n - 1, bs_sem, br_sem)
    back_sum.wait_recv()

    scope("combine")
    back_rows = back.reshape(n * SLOTS, chunks, 128)

    def combine(t, carry):
        first, second = (
            back_rows[jnp.clip(table_s[SLOTS + j, t], 0, n * SLOTS - 1)].astype(F32)
            * weight_s[j, t]
            for j in range(2)
        )
        at = pl.multiple_of(t * chunks, chunks)
        tiles32[pl.ds(at, chunks), :] = first + second
        return carry

    lax.fori_loop(0, rows, combine, 0, unroll=8)
    parts = [tiles32[pl.ds(c, rows, stride=chunks), :] for c in range(chunks)]
    combined = jnp.concatenate(parts, axis=1)
    out[...] = (residual[...] + combined * inv_rms(combined) * g_out[...]).astype(BF16)
    scope("drain")
    for done in sums:
        done.wait_send()
    back_sum.wait_send()
    count_sum.wait_send()
    scope(None)


def deliver_kernel(a, b, c, a_out, b_out, c_out, sem):
    trips = ((a, a_out), (b, b_out), (c, c_out))
    copies = [pltpu.make_async_copy(x, y, sem.at[i]) for i, (x, y) in enumerate(trips)]
    for copy in copies:
        copy.start()
    for copy in copies:
        copy.wait()


def shards(
    n,
    tokens,
    conv_state,
    recur_state,
    w_branch,
    w_gate,
    conv_taps,
    rate_blocks,
    input_blocks,
    decay_param,
    w_mix,
    gain_pre,
    gain_post,
    gain_ffn,
    gain_out,
    routes,
    affinity,
    w_expert_gate,
    w_expert_up,
    w_expert_down,
):
    rows, width = tokens.shape
    bw = recur_state.shape[1]
    ff = w_expert_gate.shape[2]
    chunks = width // 128
    vmem = pl.BlockSpec(memory_space=pltpu.VMEM)
    hbm = pl.BlockSpec(memory_space=pl.ANY)
    dma = pltpu.SemaphoreType.DMA
    inputs = (
        tokens,
        conv_state.transpose(1, 0, 2),
        recur_state,
        conv_taps,
        decay_param.reshape(1, bw),
        rate_blocks.reshape(bw, -1),
        input_blocks.reshape(bw, -1),
        gain_pre.reshape(1, width),
        gain_post.reshape(1, width),
        gain_ffn.reshape(1, width),
        gain_out.reshape(1, width),
        routes.T,
        affinity.T,
        w_branch,
        w_gate,
        w_mix,
        w_expert_gate.reshape(width, ff),
        w_expert_up.reshape(width, ff),
        w_expert_down.reshape(ff, width),
    )
    results = (
        jax.ShapeDtypeStruct((rows, width), BF16),
        jax.ShapeDtypeStruct((3, rows, bw), BF16),
        jax.ShapeDtypeStruct((rows, bw), F32),
    )
    produced = pl.pallas_call(
        functools.partial(layer_kernel, n),
        out_shape=tuple(pltpu.VMEM(x.shape, x.dtype) for x in results),
        in_specs=[hbm] * len(inputs),
        out_specs=(vmem, vmem, vmem),
        scratch_shapes=[pltpu.VMEM(x.shape, x.dtype) for x in inputs]
        + [
            pltpu.VMEM((2, 4, 256, 256), BF16),
            pltpu.VMEM((rows, width), F32),
            pltpu.VMEM((rows * chunks + chunks, 128), F32),
            pltpu.VMEM((rows, chunks, 128), BF16),
            pltpu.VMEM((n, SLOTS, chunks, 128), BF16),
            pltpu.VMEM((HALF, SLOTS, chunks, 128), BF16),
            pltpu.VMEM((HALF, SLOTS, chunks, 128), BF16),
            pltpu.VMEM((HALF, SLOTS, chunks, 128), BF16),
            pltpu.VMEM((HALF, SLOTS, chunks, 128), BF16),
            pltpu.VMEM((n, SLOTS, chunks, 128), BF16),
            pltpu.VMEM((LIMIT, width), BF16),
            pltpu.VMEM((1, n), I32),
            pltpu.VMEM((n, n), I32),
            pltpu.VMEM((8, 128), I32),
            pltpu.SMEM((8, 128), I32),
            pltpu.VMEM((8, 128), I32),
            pltpu.SMEM((8, 128), I32),
            pltpu.VMEM((8, 128), F32),
            pltpu.SMEM((8, 128), F32),
            dma((26,)),
            dma,
            dma,
            dma,
            dma((2,)),
            dma((2,)),
            dma,
            dma,
        ],
        compiler_params=pltpu.CompilerParams(
            collective_id=0, has_side_effects=True, vmem_limit_bytes=60 * 1024 * 1024
        ),
        name="layer",
    )(*inputs)
    layer_out, conv_next, state_next = pl.pallas_call(
        deliver_kernel,
        out_shape=results,
        in_specs=[vmem] * 3,
        out_specs=(hbm, hbm, hbm),
        scratch_shapes=[dma((3,))],
        name="deliver",
    )(*(pltpu.with_memory_space_constraint(x, pltpu.VMEM) for x in produced))
    return (layer_out, conv_next.transpose(1, 0, 2), state_next)


def solution(mesh):
    row, cube, whole = P("ep", None), P("ep", None, None), P()
    return jax.shard_map(
        functools.partial(shards, mesh.shape["ep"]),
        mesh=mesh,
        in_specs=(row, cube, row) + (whole,) * 11 + (row, row, cube, cube, cube),
        out_specs=(row, cube, row),
        check_vma=False,
    )
```

```python
import functools

import jax
import jax.numpy as jnp
from jax import lax
from jax.experimental import pallas as pl
from jax.experimental.pallas import tpu as pltpu
from jax.sharding import PartitionSpec as P

MESH = pl.DeviceIdType.MESH
EPS = 1e-06
DECAY = 8.0
LIMIT = 64
SLOTS = 3
F32 = jnp.float32
BF16 = jnp.bfloat16
I32 = jnp.int32


def dot(a, b):
    return jnp.dot(a, b, preferred_element_type=F32)


def inv_rms(values):
    return lax.rsqrt(jnp.mean(values * values, axis=-1, keepdims=True) + EPS)


def minus_expm1(y):
    series = y * (1.0 + y * (1 / 2 + y * (1 / 6 + y * (1 / 24 + y * (1 / 120)))))
    return -jnp.where(y > -0.1, series, jnp.exp(y) - 1.0)


SCOPES = []


def scope(name):
    if SCOPES:
        SCOPES.pop().__exit__(None, None, None)
    if name:
        SCOPES.append(jax.named_scope(name))
        SCOPES[-1].__enter__()


def moved(device, step, sign):
    z, y, x, core = step
    return (
        (((device >> 5) + sign * z) & 3) << 5
        | (((device >> 3) + sign * y) & 3) << 3
        | (((device >> 1) + sign * x) & 3) << 1
        | ((device & 1) ^ core)
    )


def step_of(half, q):
    return ((q >> 5) * 2 + (1 - half), (q >> 3) & 3, (q >> 1) & 3, q & 1)


HALF = 64
GROUP = 8
TURN = 47
TURN_BACK = 15


def layer_kernel(
    n,
    tokens_h,
    conv_h,
    recur_h,
    taps_h,
    decay_h,
    rate_h,
    input_h,
    g_pre_h,
    g_post_h,
    g_ffn_h,
    g_out_h,
    routes_h,
    affinity_h,
    wb_h,
    wg_h,
    wm_h,
    eg_h,
    eu_h,
    ed_h,
    out,
    conv_out,
    state_out,
    tokens,
    conv_in,
    recur,
    taps,
    decay,
    rate_b,
    input_b,
    g_pre,
    g_post,
    g_ffn,
    g_out,
    routes,
    affinity,
    wb,
    wg,
    wm,
    eg,
    eu,
    ed,
    bd,
    residual,
    tiles32,
    tiles,
    send,
    recv_a,
    recv_b,
    ret_a,
    ret_b,
    back,
    xb,
    counts,
    all_counts,
    table_v,
    table_s,
    meta_v,
    meta_s,
    weight_v,
    weight_s,
    w_sem,
    t_sem,
    cs_sem,
    cr_sem,
    ps_sem,
    pr_sem,
    bs_sem,
    br_sem,
):
    me = lax.axis_index("ep")
    rows, width = tokens.shape
    chunks = width // 128

    loads = {}

    def load(key, src, dst):
        loads[key] = pltpu.make_async_copy(src, dst, w_sem.at[len(loads)])
        loads[key].start()

    def ready(*keys):
        for k in keys:
            loads[k].wait()

    def load_columns(g):
        cols = pl.ds(256 * g, 256)
        load(f"wb{g}", wb_h.at[:, cols], wb.at[:, cols])
        load(f"wg{g}", wg_h.at[:, cols], wg.at[:, cols])

    load("tokens", tokens_h, tokens)
    load("g_pre", g_pre_h, g_pre)
    load("routes", routes_h, routes)
    load("rate", rate_h, rate_b)
    load("input", input_h, input_b)
    load_columns(0)
    load("conv", conv_h, conv_in)
    load("taps", taps_h, taps)
    load("decay", decay_h, decay)
    load("recur", recur_h, recur)
    load_columns(1)
    load_columns(2)
    load_columns(3)
    for h in range(2):
        part = pl.ds(512 * h, 512)
        load(f"wm{h}", wm_h.at[part], wm.at[part])
    load("g_post", g_post_h, g_post)
    load("g_ffn", g_ffn_h, g_ffn)
    load("affinity", affinity_h, affinity)
    load("g_out", g_out_h, g_out)

    scope("greet")
    barrier = pltpu.get_barrier_semaphore()

    def greet(i, carry):
        for j in range(4):
            peer = (me + 4 * i + j) & (n - 1)
            pl.semaphore_signal(barrier, inc=1, device_id=(peer,), device_id_type=MESH)
        return carry

    lax.fori_loop(1, n // 4, greet, 0)
    for j in range(1, 4):
        peer = (me + j) & (n - 1)
        pl.semaphore_signal(barrier, inc=1, device_id=(peer,), device_id_type=MESH)

    scope("norm")
    ready("tokens", "g_pre", "routes", "rate", "input")
    tok = tokens[...].astype(F32)
    normed = (tok * inv_rms(tok) * g_pre[...]).astype(BF16)
    scope("first")
    ready("wb0", "wg0", "conv", "taps", "decay", "recur")
    spread = (
        lax.broadcasted_iota(I32, (64, 256), 1) % 64 == lax.broadcasted_iota(I32, (64, 256), 0)
    ).astype(BF16)
    keep = (lax.broadcasted_iota(I32, (256, 256), 0) // 64) == (
        lax.broadcasted_iota(I32, (256, 256), 1) // 64
    )
    for k, blocks in enumerate((rate_b, input_b)):
        for g in range(4):
            wide = dot(blocks[256 * g : 256 * (g + 1), :], spread)
            bd[k, g] = jnp.where(keep, wide, 0.0).astype(BF16)

    r0, r1 = routes[0:1, :], routes[1:2, :]
    sub = lax.broadcasted_iota(I32, (rows, rows), 0)
    lane = lax.broadcasted_iota(I32, (rows, rows), 1)
    diag = sub == lane

    def column(row):
        return jnp.sum(jnp.where(diag, row, jnp.zeros_like(row)), axis=1, keepdims=True)

    def as_row(col):
        return jnp.sum(jnp.where(diag, col, jnp.zeros_like(col)), axis=0, keepdims=True)

    experts = lax.broadcasted_iota(I32, (rows, n), 1)
    token_of = lax.broadcasted_iota(I32, (rows, n), 0)
    m0, m1 = column(r0) == experts, column(r1) == experts
    both = m0 | m1
    before = dot((lane < sub).astype(F32), both.astype(F32)).astype(I32)
    counts[...] = jnp.sum(both.astype(I32), axis=0, keepdims=True)
    table_v[...] = jnp.zeros_like(table_v)
    for s in range(SLOTS):
        table_v[s : s + 1, :] = jnp.sum(
            jnp.where(both & (before == s), token_of, 0), axis=0, keepdims=True
        )
    for j, m in enumerate((m0, m1)):
        where_at = jnp.sum(jnp.where(m, experts * SLOTS + before, 0), axis=1, keepdims=True)
        table_v[SLOTS + j : SLOTS + j + 1, 0:rows] = as_row(where_at)
    table_copy = pltpu.make_async_copy(table_v, table_s, t_sem)
    table_copy.start()

    def project(g):
        cols = slice(256 * g, 256 * (g + 1))
        return dot(normed, wb[:, cols]).astype(BF16), dot(normed, wg[:, cols]).astype(BF16)

    def advance(g, branch, gate):
        cols = slice(256 * g, 256 * (g + 1))
        conv_out[0, :, cols] = conv_in[1, :, cols]
        conv_out[1, :, cols] = conv_in[2, :, cols]
        conv_out[2, :, cols] = branch
        conv = branch.astype(F32) * taps[3:4, cols]
        for k in range(3):
            conv = conv + conv_in[k, :, cols].astype(F32) * taps[k : k + 1, cols]
        conv_b = conv.astype(BF16)
        d = decay[:, cols]
        soft = jnp.maximum(-d, 0.0) + jnp.log1p(jnp.exp(-jnp.abs(d)))
        rate = jax.nn.sigmoid(dot(conv_b, bd[0, g]))
        inflow = jax.nn.sigmoid(dot(conv_b, bd[1, g]))
        log_decay = -DECAY * rate * soft
        state = jnp.exp(log_decay) * recur[:, cols] + jnp.sqrt(minus_expm1(2.0 * log_decay)) * (
            inflow * conv
        )
        state_out[:, cols] = state
        x = gate.astype(F32)
        gelu = 0.5 * x * (1.0 + jnp.tanh(0.7978845608028654 * (x + 0.044715 * (x * x * x))))
        return (state * gelu).astype(BF16)

    merged = []
    projected = project(0)
    scope("project")
    for g in range(1, 4):
        ready(f"wb{g}", f"wg{g}")
        following = project(g)
        merged.append(advance(g - 1, *projected))
        projected = following
    scope("mix")
    ready("wm0")
    half_mix = dot(jnp.concatenate(merged[:2], axis=1), wm[:512, :])
    merged.append(advance(3, *projected))
    ready("wm1", "g_post", "g_ffn")
    mix = half_mix + dot(jnp.concatenate(merged[2:], axis=1), wm[512:, :])
    mix = mix.astype(BF16).astype(F32)
    load("eg", eg_h, eg)
    load("eu", eu_h, eu)
    load("ed", ed_h, ed)
    res = tok + mix * inv_rms(mix) * g_post[...]
    residual[...] = res
    ffn = res * inv_rms(res) * g_ffn[...]

    scope("tiles")
    for c in range(chunks):
        tiles32[pl.ds(c, rows, stride=chunks), :] = ffn[:, 128 * c : 128 * (c + 1)]

    def to_tiles(t, carry):
        at = pl.multiple_of(t * chunks, chunks)
        tiles[t] = tiles32[pl.ds(at, chunks), :].astype(BF16)
        return carry

    lax.fori_loop(0, rows, to_tiles, 0, unroll=8)
    table_copy.wait()

    scope("barrier")
    pl.semaphore_wait(barrier, n - 1)
    scope("send")

    def own_tile(index):
        return tiles[jnp.clip(index, 0, rows - 1)]

    def turned(i):
        return (i * TURN) & (HALF - 1)

    def post(source, target, ssem, rsem, peer):
        pltpu.make_async_remote_copy(
            src_ref=source,
            dst_ref=target,
            send_sem=ssem,
            recv_sem=rsem,
            device_id=(peer,),
            device_id_type=MESH,
        ).start()

    def send_count(peer):
        post(counts, all_counts.at[pl.ds(me, 1)], cs_sem, cr_sem, peer)

    def piped(first, prepare, launch):
        def group(g, start, run):
            for j in range(start, GROUP):
                run(g * GROUP + j)

        def body(g, carry):
            group(g, 0, prepare)
            group(g - 1, 0, launch)
            return carry

        group(0, first, prepare)
        group(1, 0, prepare)
        group(0, first, launch)
        lax.fori_loop(2, HALF // GROUP, body, 0)
        group(HALF // GROUP - 1, 0, launch)

    def pick_rows(half, i):
        peer = moved(me, step_of(half, turned(i)), 1)
        for s in range(SLOTS):
            send[peer, s] = own_tile(table_s[s, peer])
        if half == 0:
            send_count(peer)
            if not (isinstance(i, int) and i == 0):
                send_count(moved(me, step_of(1, turned(i)), 1))

    def send_rows(half, i):
        q = turned(i)
        peer = moved(me, step_of(half, q), 1)
        target = (recv_a, recv_b)[half]
        post(send.at[peer], target.at[q], ps_sem.at[half], pr_sem.at[half], peer)

    for half in range(2):
        piped(half, functools.partial(pick_rows, half), functools.partial(send_rows, half))
    for s in range(SLOTS):
        recv_b[0, s] = own_tile(table_s[s, me])
    all_counts[pl.ds(me, 1), :] = counts[...]

    def total(buffer, blocks, ssem, rsem):
        part = buffer.at[pl.ds(0, blocks)]
        return pltpu.make_async_remote_copy(
            src_ref=part,
            dst_ref=part,
            send_sem=ssem,
            recv_sem=rsem,
            device_id=(me ^ 1,),
            device_id_type=MESH,
        )

    scope("meta")
    count_sum = total(all_counts, n - 1, cs_sem, cr_sem)
    count_sum.wait_recv()
    every = all_counts[...]
    sub_n = lax.broadcasted_iota(I32, (n, n), 0)
    lane_n = lax.broadcasted_iota(I32, (n, n), 1)
    own_col = jnp.sum(jnp.where(lane_n == me, every, 0), axis=1, keepdims=True)
    own_row = jnp.sum(jnp.where(lane_n == sub_n, own_col, 0), axis=0, keepdims=True)
    first_col = jnp.sum(jnp.where(lane_n < sub_n, own_row, 0), axis=1, keepdims=True)
    first_row = jnp.sum(jnp.where(sub_n < lane_n, own_col, 0), axis=0, keepdims=True)
    hit = (first_col <= lane_n) & (lane_n < first_col + own_col)
    step_z = ((me >> 5) - (sub_n >> 5)) & 3
    entry = (
        (step_z >> 1) << 5
        | (((me >> 3) - (sub_n >> 3)) & 3) << 3
        | (((me >> 1) - (sub_n >> 1)) & 3) << 1
        | ((me ^ sub_n) & 1)
    )
    place = SLOTS * entry + lane_n - first_col
    meta_v[...] = jnp.zeros_like(meta_v)
    for half in range(2):
        meta_v[half : half + 1, :] = jnp.sum(
            jnp.where(hit & ((step_z & 1) == 1 - half), place, 0), axis=0, keepdims=True
        )
    for s in range(SLOTS):
        meta_v[2 + s : 3 + s, :] = jnp.minimum(first_row + s, LIMIT - 1)
    meta_copy = pltpu.make_async_copy(meta_v, meta_s, t_sem)
    meta_copy.start()

    base = jnp.sum(jnp.where(sub_n < me, every, 0), axis=0, keepdims=True)
    fits = (base + before) < LIMIT
    ready("affinity")
    a0, a1 = affinity[0:1, :], affinity[1:2, :]
    weight_v[...] = jnp.zeros_like(weight_v)
    for j, (m, a) in enumerate(((m0, a0), (m1, a1))):
        kept = jnp.sum(jnp.where(m & fits, 1.0, 0.0), axis=1, keepdims=True)
        weight_v[j : j + 1, 0:rows] = as_row(kept) * (a / (a0 + a1))
    meta_copy.wait()
    weight_copy = pltpu.make_async_copy(weight_v, weight_s, t_sem)
    weight_copy.start()
    ready("eg", "eu", "ed", "g_out")

    sums = []
    for half, (got, ret) in enumerate(((recv_a, ret_a), (recv_b, ret_b))):
        scope(f"wait{half}")
        rows_sum = total(got, HALF - half, ps_sem.at[half], pr_sem.at[half])
        rows_sum.wait_recv()
        sums.append(rows_sum)
        scope(f"expert{half}")
        got_rows = got.reshape(HALF * SLOTS, chunks, 128)

        def accept(r, carry):
            at = pl.multiple_of(r * chunks, chunks)
            index = jnp.clip(meta_s[half, r], 0, HALF * SLOTS - 1)
            tiles32[pl.ds(at, chunks), :] = got_rows[index].astype(F32)
            return carry

        lax.fori_loop(0, LIMIT, accept, 0, unroll=8)
        for c in range(chunks):
            part = tiles32[pl.ds(c, LIMIT, stride=chunks), :]
            xb[:, 128 * c : 128 * (c + 1)] = part.astype(BF16)
        x = xb[...]
        hidden = (jax.nn.silu(dot(x, eg[...])) * dot(x, eu[...])).astype(BF16)
        result = dot(hidden, ed[...])
        for c in range(chunks):
            tiles32[pl.ds(c, LIMIT, stride=chunks), :] = result[:, 128 * c : 128 * (c + 1)]
        lax.fori_loop(0, LIMIT, to_tiles, 0, unroll=8)
        scope(f"give{half}")

        def result_tile(s, peer):
            return tiles[jnp.clip(meta_s[2 + s, peer], 0, LIMIT - 1)]

        step_1 = moved(me, (0, 0, 0, 1), 1)
        q_1 = (step_1 >> 6) << 5 | (step_1 & 31)
        lead = (q_1 * TURN_BACK) & (HALF - 1)
        lead = jnp.where(lead < half, half, lead)

        def turned_back(i):
            return turned(jnp.where(i == half, lead, jnp.where(i == lead, half, i)))

        def give(i):
            q = turned_back(i)
            peer = moved(me, step_of(half, q), -1)
            for s in range(SLOTS):
                ret[q, s] = result_tile(s, peer)

        def send_back(i):
            q = turned_back(i)
            peer = moved(me, step_of(half, q), -1)
            post(ret.at[q], back.at[me], bs_sem, br_sem, peer)

        piped(half, give, send_back)
    for s in range(SLOTS):
        back[me, s] = result_tile(s, me)
    weight_copy.wait()
    scope("wait2")
    back_sum = total(back, n - 1, bs_sem, br_sem)
    back_sum.wait_recv()

    scope("combine")
    back_rows = back.reshape(n * SLOTS, chunks, 128)

    def combine(t, carry):
        first, second = (
            back_rows[jnp.clip(table_s[SLOTS + j, t], 0, n * SLOTS - 1)].astype(F32)
            * weight_s[j, t]
            for j in range(2)
        )
        at = pl.multiple_of(t * chunks, chunks)
        tiles32[pl.ds(at, chunks), :] = first + second
        return carry

    lax.fori_loop(0, rows, combine, 0, unroll=8)
    parts = [tiles32[pl.ds(c, rows, stride=chunks), :] for c in range(chunks)]
    combined = jnp.concatenate(parts, axis=1)
    out[...] = (residual[...] + combined * inv_rms(combined) * g_out[...]).astype(BF16)
    scope("drain")
    for done in sums:
        done.wait_send()
    back_sum.wait_send()
    count_sum.wait_send()
    scope(None)


def deliver_kernel(a, b, c, a_out, b_out, c_out, sem):
    trips = ((a, a_out), (b, b_out), (c, c_out))
    copies = [pltpu.make_async_copy(x, y, sem.at[i]) for i, (x, y) in enumerate(trips)]
    for copy in copies:
        copy.start()
    for copy in copies:
        copy.wait()


def shards(
    n,
    tokens,
    conv_state,
    recur_state,
    w_branch,
    w_gate,
    conv_taps,
    rate_blocks,
    input_blocks,
    decay_param,
    w_mix,
    gain_pre,
    gain_post,
    gain_ffn,
    gain_out,
    routes,
    affinity,
    w_expert_gate,
    w_expert_up,
    w_expert_down,
):
    rows, width = tokens.shape
    bw = recur_state.shape[1]
    ff = w_expert_gate.shape[2]
    chunks = width // 128
    vmem = pl.BlockSpec(memory_space=pltpu.VMEM)
    hbm = pl.BlockSpec(memory_space=pl.ANY)
    dma = pltpu.SemaphoreType.DMA
    inputs = (
        tokens,
        conv_state.transpose(1, 0, 2),
        recur_state,
        conv_taps,
        decay_param.reshape(1, bw),
        rate_blocks.reshape(bw, -1),
        input_blocks.reshape(bw, -1),
        gain_pre.reshape(1, width),
        gain_post.reshape(1, width),
        gain_ffn.reshape(1, width),
        gain_out.reshape(1, width),
        routes.T,
        affinity.T,
        w_branch,
        w_gate,
        w_mix,
        w_expert_gate.reshape(width, ff),
        w_expert_up.reshape(width, ff),
        w_expert_down.reshape(ff, width),
    )
    results = (
        jax.ShapeDtypeStruct((rows, width), BF16),
        jax.ShapeDtypeStruct((3, rows, bw), BF16),
        jax.ShapeDtypeStruct((rows, bw), F32),
    )
    produced = pl.pallas_call(
        functools.partial(layer_kernel, n),
        out_shape=tuple(pltpu.VMEM(x.shape, x.dtype) for x in results),
        in_specs=[hbm] * len(inputs),
        out_specs=(vmem, vmem, vmem),
        scratch_shapes=[pltpu.VMEM(x.shape, x.dtype) for x in inputs]
        + [
            pltpu.VMEM((2, 4, 256, 256), BF16),
            pltpu.VMEM((rows, width), F32),
            pltpu.VMEM((rows * chunks + chunks, 128), F32),
            pltpu.VMEM((rows, chunks, 128), BF16),
            pltpu.VMEM((n, SLOTS, chunks, 128), BF16),
            pltpu.VMEM((HALF, SLOTS, chunks, 128), BF16),
            pltpu.VMEM((HALF, SLOTS, chunks, 128), BF16),
            pltpu.VMEM((HALF, SLOTS, chunks, 128), BF16),
            pltpu.VMEM((HALF, SLOTS, chunks, 128), BF16),
            pltpu.VMEM((n, SLOTS, chunks, 128), BF16),
            pltpu.VMEM((LIMIT, width), BF16),
            pltpu.VMEM((1, n), I32),
            pltpu.VMEM((n, n), I32),
            pltpu.VMEM((8, 128), I32),
            pltpu.SMEM((8, 128), I32),
            pltpu.VMEM((8, 128), I32),
            pltpu.SMEM((8, 128), I32),
            pltpu.VMEM((8, 128), F32),
            pltpu.SMEM((8, 128), F32),
            dma((26,)),
            dma,
            dma,
            dma,
            dma((2,)),
            dma((2,)),
            dma,
            dma,
        ],
        compiler_params=pltpu.CompilerParams(
            collective_id=0, has_side_effects=True, vmem_limit_bytes=60 * 1024 * 1024
        ),
        name="layer",
    )(*inputs)
    layer_out, conv_next, state_next = pl.pallas_call(
        deliver_kernel,
        out_shape=results,
        in_specs=[vmem] * 3,
        out_specs=(hbm, hbm, hbm),
        scratch_shapes=[dma((3,))],
        name="deliver",
    )(*(pltpu.with_memory_space_constraint(x, pltpu.VMEM) for x in produced))
    return (layer_out, conv_next.transpose(1, 0, 2), state_next)


def solution(mesh):
    row, cube, whole = P("ep", None), P("ep", None, None), P()
    return jax.shard_map(
        functools.partial(shards, mesh.shape["ep"]),
        mesh=mesh,
        in_specs=(row, cube, row) + (whole,) * 11 + (row, row, cube, cube, cube),
        out_specs=(row, cube, row),
        check_vma=False,
    )
```

```python
import functools

import jax
import jax.numpy as jnp
from jax import lax
from jax.experimental import pallas as pl
from jax.experimental.pallas import tpu as pltpu
from jax.sharding import PartitionSpec as P

MESH = pl.DeviceIdType.MESH
EPS = 1e-06
DECAY = 8.0
LIMIT = 64
SLOTS = 3
F32 = jnp.float32
BF16 = jnp.bfloat16
I32 = jnp.int32


def dot(a, b):
    return jnp.dot(a, b, preferred_element_type=F32)


def inv_rms(values):
    return lax.rsqrt(jnp.mean(values * values, axis=-1, keepdims=True) + EPS)


def minus_expm1(y):
    series = y * (1.0 + y * (1 / 2 + y * (1 / 6 + y * (1 / 24 + y * (1 / 120)))))
    return -jnp.where(y > -0.1, series, jnp.exp(y) - 1.0)


SCOPES = []


def scope(name):
    if SCOPES:
        SCOPES.pop().__exit__(None, None, None)
    if name:
        SCOPES.append(jax.named_scope(name))
        SCOPES[-1].__enter__()


def moved(device, step, sign):
    z, y, x, core = step
    return (
        (((device >> 5) + sign * z) & 3) << 5
        | (((device >> 3) + sign * y) & 3) << 3
        | (((device >> 1) + sign * x) & 3) << 1
        | ((device & 1) ^ core)
    )


def step_of(half, q):
    return ((q >> 5) * 2 + (1 - half), (q >> 3) & 3, (q >> 1) & 3, q & 1)


HALF = 64
GROUP = 4
TURN = 47
TURN_BACK = 15


def layer_kernel(
    n,
    tokens_h,
    conv_h,
    recur_h,
    taps_h,
    decay_h,
    rate_h,
    input_h,
    g_pre_h,
    g_post_h,
    g_ffn_h,
    g_out_h,
    routes_h,
    affinity_h,
    wb_h,
    wg_h,
    wm_h,
    eg_h,
    eu_h,
    ed_h,
    out,
    conv_out,
    state_out,
    tokens,
    conv_in,
    recur,
    taps,
    decay,
    rate_b,
    input_b,
    g_pre,
    g_post,
    g_ffn,
    g_out,
    routes,
    affinity,
    wb,
    wg,
    wm,
    eg,
    eu,
    ed,
    bd,
    residual,
    tiles32,
    tiles,
    send,
    recv_a,
    recv_b,
    ret_a,
    ret_b,
    back,
    xb,
    counts,
    all_counts,
    table_v,
    table_s,
    meta_v,
    meta_s,
    weight_v,
    weight_s,
    w_sem,
    t_sem,
    cs_sem,
    cr_sem,
    ps_sem,
    pr_sem,
    bs_sem,
    br_sem,
):
    me = lax.axis_index("ep")
    rows, width = tokens.shape
    chunks = width // 128

    loads = {}

    def load(key, src, dst):
        loads[key] = pltpu.make_async_copy(src, dst, w_sem.at[len(loads)])
        loads[key].start()

    def ready(*keys):
        for k in keys:
            loads[k].wait()

    def load_columns(g):
        cols = pl.ds(256 * g, 256)
        load(f"wb{g}", wb_h.at[:, cols], wb.at[:, cols])
        load(f"wg{g}", wg_h.at[:, cols], wg.at[:, cols])

    load("tokens", tokens_h, tokens)
    load("g_pre", g_pre_h, g_pre)
    load("routes", routes_h, routes)
    load("rate", rate_h, rate_b)
    load("input", input_h, input_b)
    load_columns(0)
    load("conv", conv_h, conv_in)
    load("taps", taps_h, taps)
    load("decay", decay_h, decay)
    load("recur", recur_h, recur)
    load_columns(1)
    load_columns(2)
    load_columns(3)
    for h in range(2):
        part = pl.ds(512 * h, 512)
        load(f"wm{h}", wm_h.at[part], wm.at[part])
    load("g_post", g_post_h, g_post)
    load("g_ffn", g_ffn_h, g_ffn)
    load("affinity", affinity_h, affinity)
    load("g_out", g_out_h, g_out)

    scope("greet")
    barrier = pltpu.get_barrier_semaphore()

    def greet(i, carry):
        for j in range(4):
            peer = (me + 4 * i + j) & (n - 1)
            pl.semaphore_signal(barrier, inc=1, device_id=(peer,), device_id_type=MESH)
        return carry

    lax.fori_loop(1, n // 4, greet, 0)
    for j in range(1, 4):
        peer = (me + j) & (n - 1)
        pl.semaphore_signal(barrier, inc=1, device_id=(peer,), device_id_type=MESH)

    scope("norm")
    ready("tokens", "g_pre", "routes", "rate", "input")
    tok = tokens[...].astype(F32)
    normed = (tok * inv_rms(tok) * g_pre[...]).astype(BF16)
    scope("first")
    ready("wb0", "wg0", "conv", "taps", "decay", "recur")
    spread = (
        lax.broadcasted_iota(I32, (64, 256), 1) % 64 == lax.broadcasted_iota(I32, (64, 256), 0)
    ).astype(BF16)
    keep = (lax.broadcasted_iota(I32, (256, 256), 0) // 64) == (
        lax.broadcasted_iota(I32, (256, 256), 1) // 64
    )
    for k, blocks in enumerate((rate_b, input_b)):
        for g in range(4):
            wide = dot(blocks[256 * g : 256 * (g + 1), :], spread)
            bd[k, g] = jnp.where(keep, wide, 0.0).astype(BF16)

    r0, r1 = routes[0:1, :], routes[1:2, :]
    sub = lax.broadcasted_iota(I32, (rows, rows), 0)
    lane = lax.broadcasted_iota(I32, (rows, rows), 1)
    diag = sub == lane

    def column(row):
        return jnp.sum(jnp.where(diag, row, jnp.zeros_like(row)), axis=1, keepdims=True)

    def as_row(col):
        return jnp.sum(jnp.where(diag, col, jnp.zeros_like(col)), axis=0, keepdims=True)

    experts = lax.broadcasted_iota(I32, (rows, n), 1)
    token_of = lax.broadcasted_iota(I32, (rows, n), 0)
    m0, m1 = column(r0) == experts, column(r1) == experts
    both = m0 | m1
    before = dot((lane < sub).astype(F32), both.astype(F32)).astype(I32)
    counts[...] = jnp.sum(both.astype(I32), axis=0, keepdims=True)
    table_v[...] = jnp.zeros_like(table_v)
    for s in range(SLOTS):
        table_v[s : s + 1, :] = jnp.sum(
            jnp.where(both & (before == s), token_of, 0), axis=0, keepdims=True
        )
    for j, m in enumerate((m0, m1)):
        where_at = jnp.sum(jnp.where(m, experts * SLOTS + before, 0), axis=1, keepdims=True)
        table_v[SLOTS + j : SLOTS + j + 1, 0:rows] = as_row(where_at)
    table_copy = pltpu.make_async_copy(table_v, table_s, t_sem)
    table_copy.start()

    def project(g):
        cols = slice(256 * g, 256 * (g + 1))
        return dot(normed, wb[:, cols]).astype(BF16), dot(normed, wg[:, cols]).astype(BF16)

    def advance(g, branch, gate):
        cols = slice(256 * g, 256 * (g + 1))
        conv_out[0, :, cols] = conv_in[1, :, cols]
        conv_out[1, :, cols] = conv_in[2, :, cols]
        conv_out[2, :, cols] = branch
        conv = branch.astype(F32) * taps[3:4, cols]
        for k in range(3):
            conv = conv + conv_in[k, :, cols].astype(F32) * taps[k : k + 1, cols]
        conv_b = conv.astype(BF16)
        d = decay[:, cols]
        soft = jnp.maximum(-d, 0.0) + jnp.log1p(jnp.exp(-jnp.abs(d)))
        rate = jax.nn.sigmoid(dot(conv_b, bd[0, g]))
        inflow = jax.nn.sigmoid(dot(conv_b, bd[1, g]))
        log_decay = -DECAY * rate * soft
        state = jnp.exp(log_decay) * recur[:, cols] + jnp.sqrt(minus_expm1(2.0 * log_decay)) * (
            inflow * conv
        )
        state_out[:, cols] = state
        x = gate.astype(F32)
        gelu = 0.5 * x * (1.0 + jnp.tanh(0.7978845608028654 * (x + 0.044715 * (x * x * x))))
        return (state * gelu).astype(BF16)

    merged = []
    projected = project(0)
    scope("project")
    for g in range(1, 4):
        ready(f"wb{g}", f"wg{g}")
        following = project(g)
        merged.append(advance(g - 1, *projected))
        projected = following
    scope("mix")
    ready("wm0")
    half_mix = dot(jnp.concatenate(merged[:2], axis=1), wm[:512, :])
    merged.append(advance(3, *projected))
    ready("wm1", "g_post", "g_ffn")
    mix = half_mix + dot(jnp.concatenate(merged[2:], axis=1), wm[512:, :])
    mix = mix.astype(BF16).astype(F32)
    load("eg", eg_h, eg)
    load("eu", eu_h, eu)
    load("ed", ed_h, ed)
    res = tok + mix * inv_rms(mix) * g_post[...]
    residual[...] = res
    ffn = res * inv_rms(res) * g_ffn[...]

    scope("tiles")
    for c in range(chunks):
        tiles32[pl.ds(c, rows, stride=chunks), :] = ffn[:, 128 * c : 128 * (c + 1)]

    def to_tiles(t, carry):
        at = pl.multiple_of(t * chunks, chunks)
        tiles[t] = tiles32[pl.ds(at, chunks), :].astype(BF16)
        return carry

    lax.fori_loop(0, rows, to_tiles, 0, unroll=8)
    table_copy.wait()

    scope("barrier")
    pl.semaphore_wait(barrier, n - 1)
    scope("send")

    def own_tile(index):
        return tiles[jnp.clip(index, 0, rows - 1)]

    def turned(i):
        return (i * TURN) & (HALF - 1)

    def post(source, target, ssem, rsem, peer):
        pltpu.make_async_remote_copy(
            src_ref=source,
            dst_ref=target,
            send_sem=ssem,
            recv_sem=rsem,
            device_id=(peer,),
            device_id_type=MESH,
        ).start()

    def send_count(peer):
        post(counts, all_counts.at[pl.ds(me, 1)], cs_sem, cr_sem, peer)

    def piped(first, prepare, launch):
        def group(g, start, run):
            for j in range(start, GROUP):
                run(g * GROUP + j)

        def body(g, carry):
            group(g, 0, prepare)
            group(g - 1, 0, launch)
            return carry

        group(0, first, prepare)
        group(1, 0, prepare)
        group(0, first, launch)
        lax.fori_loop(2, HALF // GROUP, body, 0)
        group(HALF // GROUP - 1, 0, launch)

    def pick_rows(half, i):
        peer = moved(me, step_of(half, turned(i)), 1)
        for s in range(SLOTS):
            send[peer, s] = own_tile(table_s[s, peer])
        if half == 0:
            send_count(peer)
            if not (isinstance(i, int) and i == 0):
                send_count(moved(me, step_of(1, turned(i)), 1))

    def send_rows(half, i):
        q = turned(i)
        peer = moved(me, step_of(half, q), 1)
        target = (recv_a, recv_b)[half]
        post(send.at[peer], target.at[q], ps_sem.at[half], pr_sem.at[half], peer)

    for half in range(2):
        piped(half, functools.partial(pick_rows, half), functools.partial(send_rows, half))
    for s in range(SLOTS):
        recv_b[0, s] = own_tile(table_s[s, me])
    all_counts[pl.ds(me, 1), :] = counts[...]

    def total(buffer, blocks, ssem, rsem):
        part = buffer.at[pl.ds(0, blocks)]
        return pltpu.make_async_remote_copy(
            src_ref=part,
            dst_ref=part,
            send_sem=ssem,
            recv_sem=rsem,
            device_id=(me ^ 1,),
            device_id_type=MESH,
        )

    scope("meta")
    count_sum = total(all_counts, n - 1, cs_sem, cr_sem)
    count_sum.wait_recv()
    every = all_counts[...]
    sub_n = lax.broadcasted_iota(I32, (n, n), 0)
    lane_n = lax.broadcasted_iota(I32, (n, n), 1)
    own_col = jnp.sum(jnp.where(lane_n == me, every, 0), axis=1, keepdims=True)
    own_row = jnp.sum(jnp.where(lane_n == sub_n, own_col, 0), axis=0, keepdims=True)
    first_col = jnp.sum(jnp.where(lane_n < sub_n, own_row, 0), axis=1, keepdims=True)
    first_row = jnp.sum(jnp.where(sub_n < lane_n, own_col, 0), axis=0, keepdims=True)
    hit = (first_col <= lane_n) & (lane_n < first_col + own_col)
    step_z = ((me >> 5) - (sub_n >> 5)) & 3
    entry = (
        (step_z >> 1) << 5
        | (((me >> 3) - (sub_n >> 3)) & 3) << 3
        | (((me >> 1) - (sub_n >> 1)) & 3) << 1
        | ((me ^ sub_n) & 1)
    )
    place = SLOTS * entry + lane_n - first_col
    meta_v[...] = jnp.zeros_like(meta_v)
    for half in range(2):
        meta_v[half : half + 1, :] = jnp.sum(
            jnp.where(hit & ((step_z & 1) == 1 - half), place, 0), axis=0, keepdims=True
        )
    for s in range(SLOTS):
        meta_v[2 + s : 3 + s, :] = jnp.minimum(first_row + s, LIMIT - 1)
    meta_copy = pltpu.make_async_copy(meta_v, meta_s, t_sem)
    meta_copy.start()

    base = jnp.sum(jnp.where(sub_n < me, every, 0), axis=0, keepdims=True)
    fits = (base + before) < LIMIT
    ready("affinity")
    a0, a1 = affinity[0:1, :], affinity[1:2, :]
    weight_v[...] = jnp.zeros_like(weight_v)
    for j, (m, a) in enumerate(((m0, a0), (m1, a1))):
        kept = jnp.sum(jnp.where(m & fits, 1.0, 0.0), axis=1, keepdims=True)
        weight_v[j : j + 1, 0:rows] = as_row(kept) * (a / (a0 + a1))
    meta_copy.wait()
    weight_copy = pltpu.make_async_copy(weight_v, weight_s, t_sem)
    weight_copy.start()
    ready("eg", "eu", "ed", "g_out")

    sums = []
    for half, (got, ret) in enumerate(((recv_a, ret_a), (recv_b, ret_b))):
        scope(f"wait{half}")
        rows_sum = total(got, HALF - half, ps_sem.at[half], pr_sem.at[half])
        rows_sum.wait_recv()
        sums.append(rows_sum)
        scope(f"expert{half}")
        got_rows = got.reshape(HALF * SLOTS, chunks, 128)

        def accept(r, carry):
            at = pl.multiple_of(r * chunks, chunks)
            index = jnp.clip(meta_s[half, r], 0, HALF * SLOTS - 1)
            tiles32[pl.ds(at, chunks), :] = got_rows[index].astype(F32)
            return carry

        lax.fori_loop(0, LIMIT, accept, 0, unroll=8)
        for c in range(chunks):
            part = tiles32[pl.ds(c, LIMIT, stride=chunks), :]
            xb[:, 128 * c : 128 * (c + 1)] = part.astype(BF16)
        x = xb[...]
        hidden = (jax.nn.silu(dot(x, eg[...])) * dot(x, eu[...])).astype(BF16)
        result = dot(hidden, ed[...])
        for c in range(chunks):
            tiles32[pl.ds(c, LIMIT, stride=chunks), :] = result[:, 128 * c : 128 * (c + 1)]
        lax.fori_loop(0, LIMIT, to_tiles, 0, unroll=8)
        scope(f"give{half}")

        def result_tile(s, peer):
            return tiles[jnp.clip(meta_s[2 + s, peer], 0, LIMIT - 1)]

        step_1 = moved(me, (0, 0, 0, 1), 1)
        q_1 = (step_1 >> 6) << 5 | (step_1 & 31)
        lead = (q_1 * TURN_BACK) & (HALF - 1)
        lead = jnp.where(lead < half, half, lead)

        def turned_back(i):
            return turned(jnp.where(i == half, lead, jnp.where(i == lead, half, i)))

        def give(i):
            q = turned_back(i)
            peer = moved(me, step_of(half, q), -1)
            for s in range(SLOTS):
                ret[q, s] = result_tile(s, peer)

        def send_back(i):
            q = turned_back(i)
            peer = moved(me, step_of(half, q), -1)
            post(ret.at[q], back.at[me], bs_sem, br_sem, peer)

        piped(half, give, send_back)
    for s in range(SLOTS):
        back[me, s] = result_tile(s, me)
    weight_copy.wait()
    scope("wait2")
    back_sum = total(back, n - 1, bs_sem, br_sem)
    back_sum.wait_recv()

    scope("combine")
    back_rows = back.reshape(n * SLOTS, chunks, 128)

    def combine(t, carry):
        first, second = (
            back_rows[jnp.clip(table_s[SLOTS + j, t], 0, n * SLOTS - 1)].astype(F32)
            * weight_s[j, t]
            for j in range(2)
        )
        at = pl.multiple_of(t * chunks, chunks)
        tiles32[pl.ds(at, chunks), :] = first + second
        return carry

    lax.fori_loop(0, rows, combine, 0, unroll=8)
    parts = [tiles32[pl.ds(c, rows, stride=chunks), :] for c in range(chunks)]
    combined = jnp.concatenate(parts, axis=1)
    out[...] = (residual[...] + combined * inv_rms(combined) * g_out[...]).astype(BF16)
    scope("drain")
    for done in sums:
        done.wait_send()
    back_sum.wait_send()
    count_sum.wait_send()
    scope(None)


def deliver_kernel(a, b, c, a_out, b_out, c_out, sem):
    trips = ((a, a_out), (b, b_out), (c, c_out))
    copies = [pltpu.make_async_copy(x, y, sem.at[i]) for i, (x, y) in enumerate(trips)]
    for copy in copies:
        copy.start()
    for copy in copies:
        copy.wait()


def shards(
    n,
    tokens,
    conv_state,
    recur_state,
    w_branch,
    w_gate,
    conv_taps,
    rate_blocks,
    input_blocks,
    decay_param,
    w_mix,
    gain_pre,
    gain_post,
    gain_ffn,
    gain_out,
    routes,
    affinity,
    w_expert_gate,
    w_expert_up,
    w_expert_down,
):
    rows, width = tokens.shape
    bw = recur_state.shape[1]
    ff = w_expert_gate.shape[2]
    chunks = width // 128
    vmem = pl.BlockSpec(memory_space=pltpu.VMEM)
    hbm = pl.BlockSpec(memory_space=pl.ANY)
    dma = pltpu.SemaphoreType.DMA
    inputs = (
        tokens,
        conv_state.transpose(1, 0, 2),
        recur_state,
        conv_taps,
        decay_param.reshape(1, bw),
        rate_blocks.reshape(bw, -1),
        input_blocks.reshape(bw, -1),
        gain_pre.reshape(1, width),
        gain_post.reshape(1, width),
        gain_ffn.reshape(1, width),
        gain_out.reshape(1, width),
        routes.T,
        affinity.T,
        w_branch,
        w_gate,
        w_mix,
        w_expert_gate.reshape(width, ff),
        w_expert_up.reshape(width, ff),
        w_expert_down.reshape(ff, width),
    )
    results = (
        jax.ShapeDtypeStruct((rows, width), BF16),
        jax.ShapeDtypeStruct((3, rows, bw), BF16),
        jax.ShapeDtypeStruct((rows, bw), F32),
    )
    produced = pl.pallas_call(
        functools.partial(layer_kernel, n),
        out_shape=tuple(pltpu.VMEM(x.shape, x.dtype) for x in results),
        in_specs=[hbm] * len(inputs),
        out_specs=(vmem, vmem, vmem),
        scratch_shapes=[pltpu.VMEM(x.shape, x.dtype) for x in inputs]
        + [
            pltpu.VMEM((2, 4, 256, 256), BF16),
            pltpu.VMEM((rows, width), F32),
            pltpu.VMEM((rows * chunks + chunks, 128), F32),
            pltpu.VMEM((rows, chunks, 128), BF16),
            pltpu.VMEM((n, SLOTS, chunks, 128), BF16),
            pltpu.VMEM((HALF, SLOTS, chunks, 128), BF16),
            pltpu.VMEM((HALF, SLOTS, chunks, 128), BF16),
            pltpu.VMEM((HALF, SLOTS, chunks, 128), BF16),
            pltpu.VMEM((HALF, SLOTS, chunks, 128), BF16),
            pltpu.VMEM((n, SLOTS, chunks, 128), BF16),
            pltpu.VMEM((LIMIT, width), BF16),
            pltpu.VMEM((1, n), I32),
            pltpu.VMEM((n, n), I32),
            pltpu.VMEM((8, 128), I32),
            pltpu.SMEM((8, 128), I32),
            pltpu.VMEM((8, 128), I32),
            pltpu.SMEM((8, 128), I32),
            pltpu.VMEM((8, 128), F32),
            pltpu.SMEM((8, 128), F32),
            dma((26,)),
            dma,
            dma,
            dma,
            dma((2,)),
            dma((2,)),
            dma,
            dma,
        ],
        compiler_params=pltpu.CompilerParams(
            collective_id=0, has_side_effects=True, vmem_limit_bytes=60 * 1024 * 1024
        ),
        name="layer",
    )(*inputs)
    layer_out, conv_next, state_next = pl.pallas_call(
        deliver_kernel,
        out_shape=results,
        in_specs=[vmem] * 3,
        out_specs=(hbm, hbm, hbm),
        scratch_shapes=[dma((3,))],
        name="deliver",
    )(*(pltpu.with_memory_space_constraint(x, pltpu.VMEM) for x in produced))
    return (layer_out, conv_next.transpose(1, 0, 2), state_next)


def solution(mesh):
    row, cube, whole = P("ep", None), P("ep", None, None), P()
    return jax.shard_map(
        functools.partial(shards, mesh.shape["ep"]),
        mesh=mesh,
        in_specs=(row, cube, row) + (whole,) * 11 + (row, row, cube, cube, cube),
        out_specs=(row, cube, row),
        check_vma=False,
    )
```
